256 devices in a mesh: grp: 2 (over y), sp: 32 (over z, core), tp: 4 (over x).
Axes of the slice: x: 4, y: 2, z: 16, core: 2. Of those that a mesh axis runs over, the one named last changes fastest.
The devices are a block of a 4x16x16 slice.
Arguments:
- residual: bfloat16 [45056, 2048], P(('grp', 'sp')), parts along dimension 0, may hold values from -6 to 6
- mix_input: bfloat16 [45056, 2048], P(('grp', 'sp'), 'tp'), parts along dimension 0, may hold values from -6 to 6
- gate_input: bfloat16 [45056, 2048], P(('grp', 'sp'), 'tp'), parts along dimension 0, may hold values from -6 to 6
- mix_kernel: bfloat16 [4, 2048], P(None, 'tp'), may hold values from -3 to 3
- recur_gate_map: bfloat16 [16, 128, 128], P('tp'), may hold values from -0.5 to 0.5
- input_gate_map: bfloat16 [16, 128, 128], P('tp'), may hold values from -0.5 to 0.5
- decay_param: float32 [2048], P('tp')
- jump_log: float32 [45056, 2048], P(('grp', 'sp'), 'tp'), parts along dimension 0, may hold values from -2.1 to 0
- out_weight: bfloat16 [2048, 2048], P('tp'), may hold values from -0.125 to 0.125
- mix_gain: float32 [2048], replicated, may hold values from 0.1 to 1.9
- inner_gain: float32 [2048], replicated, may hold values from 0.1 to 1.9
- final_gain: float32 [2048], replicated, may hold values from 0.1 to 1.9
- gate_weight: bfloat16 [2048, 5632], P('sp', 'tp'), may hold values from -0.125 to 0.125
- value_weight: bfloat16 [2048, 5632], P('sp', 'tp'), may hold values from -0.125 to 0.125
- gate_kernel: bfloat16 [3, 5632], P(None, 'tp'), may hold values from -3.5 to 3.5
- value_kernel: bfloat16 [3, 5632], P(None, 'tp'), may hold values from -3.5 to 3.5
- down_weight: bfloat16 [5632, 2048], P('tp', 'sp'), may hold values from -0.078125 to 0.078125
Outputs:
- layer_output: bfloat16 [45056, 2048], P(('grp', 'sp', 'tp')), parts along dimension 0
The draws below stay inside these ranges and needn't reach their ends.
There are 2 independent parts, one for each index of `grp`. The reference program is written for one: setup_inputs(seed, part) draws one part's arguments, and reference() takes and returns one part's arrays. A program takes and returns all parts, laid end to end along the dimension named above; an argument that names none is the same for every part. Nothing has to cross between parts.
All inputs are finite; a program needn't handle non-finite values.
Results may differ from the reference program's by a relative error of at most 0.02.
Values may be sent and summed in bfloat16 or wider, within the bound.
No kernel may reach another device: no remote copies, remote signals or barrier semaphores. Data moves between devices by JAX's collectives and lax.ppermute only.
A program may use at most 128 MiB of HBM per device.

```python
import jax
import jax.numpy as jnp
from jax import lax

D = 2048
BW = 128
NB = 16
FF = 5632
MIX_TAPS = 4
HIDDEN_TAPS = 3
TOK_DEV = 704
TOKENS = 22528
N_TP = 4


def draw_decay_param(key, part):
    fast_share = 0.5
    fast = jax.random.uniform(jax.random.fold_in(key, 11), (D,), jnp.float32) < fast_share
    fast_rate = jnp.exp(jax.random.uniform(jax.random.fold_in(key, 12), (D,), jnp.float32, jnp.log(0.008), jnp.log(0.03)))
    slow_rate = jnp.exp(jax.random.uniform(jax.random.fold_in(key, 13), (D,), jnp.float32, jnp.log(0.03), jnp.log(0.12))) / TOKENS
    rate = jnp.where(fast, fast_rate, slow_rate)
    return (-jnp.log(jnp.expm1(rate))).astype(jnp.float32)


def draw_jump_log(key, part):
    block_count = TOKENS // TOK_DEV
    factor = jnp.exp(jax.random.uniform(jax.random.fold_in(key, 21), (block_count, D), jnp.float32, jnp.log(0.3), jnp.log(3.0)))
    steady = jnp.repeat(-0.3 * factor / TOKENS, TOK_DEV, axis=0)
    spots = jax.random.randint(jax.random.fold_in(key, 22), (3,), 0, TOKENS)
    depth = jnp.log(jax.random.uniform(jax.random.fold_in(key, 23), (3, D), jnp.float32, 0.5, 0.8))
    hits = (jnp.arange(TOKENS)[:, None] == spots[None, :]).astype(jnp.float32)
    return (steady + jnp.dot(hits, depth)).astype(jnp.float32)


def block_levels(own_key, extent, pieces, low, high):
    loudness, own = 1.0, jax.random.fold_in(own_key, 6)
    for axis_at, shards_of in pieces:
        heights = jnp.exp(jax.random.uniform(jax.random.fold_in(own, axis_at), (shards_of,), jnp.float32, low / len(pieces), high / len(pieces)))
        loudness = loudness * jnp.repeat(heights, extent[axis_at] // shards_of).reshape([-1 if axis == axis_at else 1 for axis in range(len(extent))])
    return loudness


def normal_values(rng, shape, scale, limit, pieces=(), dtype=jnp.bfloat16):
    entries = scale * jax.random.normal(rng, shape, jnp.float32)
    if pieces:
        entries = entries * block_levels(rng, shape, pieces, -0.22, 0.18)
    return jnp.clip(entries, -limit, limit).astype(dtype)


def setup_inputs(seed: int = 0, part: int = 0) -> dict:
    key_of = jax.random.split(jax.random.key(seed), 18)
    part_keys = jax.random.split(jax.random.fold_in(key_of[17], part), 18)
    return {
        "residual": normal_values(part_keys[0], (TOKENS, D), 1.0, 6.0, ((0, 32),)),
        "mix_input": normal_values(part_keys[1], (TOKENS, D), 1.0, 6.0, ((0, 32), (1, 4))),
        "gate_input": normal_values(part_keys[2], (TOKENS, D), 1.0, 6.0, ((0, 32), (1, 4))),
        "mix_kernel": normal_values(key_of[3], (MIX_TAPS, D), MIX_TAPS ** -0.5, 3.0, ((1, 4),)),
        "recur_gate_map": normal_values(key_of[4], (NB, BW, BW), BW ** -0.5, 0.5, ((0, 4),)),
        "input_gate_map": normal_values(key_of[5], (NB, BW, BW), BW ** -0.5, 0.5, ((0, 4),)),
        "decay_param": draw_decay_param(jax.random.fold_in(key_of[17], 71), part),
        "jump_log": draw_jump_log(jax.random.fold_in(jax.random.fold_in(key_of[17], part), 71), part),
        "out_weight": normal_values(key_of[8], (D, D), D ** -0.5, 0.125, ((0, 4),)),
        "mix_gain": jnp.clip(1.0 + 0.18 * jax.random.normal(key_of[9], (D,), jnp.float32), 0.1, 1.9),
        "inner_gain": jnp.clip(1.0 + 0.18 * jax.random.normal(key_of[10], (D,), jnp.float32), 0.1, 1.9),
        "final_gain": jnp.clip(1.0 + 0.18 * jax.random.normal(key_of[11], (D,), jnp.float32), 0.1, 1.9),
        "gate_weight": normal_values(key_of[12], (D, FF), D ** -0.5, 0.125, ((0, 32), (1, 4))),
        "value_weight": normal_values(key_of[13], (D, FF), D ** -0.5, 0.125, ((0, 32), (1, 4))),
        "gate_kernel": normal_values(key_of[14], (HIDDEN_TAPS, FF), HIDDEN_TAPS ** -0.5, 3.5, ((1, 4),)),
        "value_kernel": normal_values(key_of[15], (HIDDEN_TAPS, FF), HIDDEN_TAPS ** -0.5, 3.5, ((1, 4),)),
        "down_weight": normal_values(key_of[16], (FF, D), FF ** -0.5, 0.078125, ((0, 4), (1, 32))),
    }


EPS = 1e-06
GATE_SCALE = 8.0

def norm_scale(values, gain_vec):
    values = values.astype(jnp.float32)
    return values * lax.rsqrt(lax.optimization_barrier(jnp.mean(values * values, axis=-1, keepdims=True)) + EPS) * gain_vec

def causal_taps(padded, kernel, length):
    kernel = kernel.astype(jnp.float32)
    result = jnp.zeros((length, padded.shape[1]), jnp.float32)
    for offset in range(kernel.shape[0]):
        result = result + padded[offset:offset + length] * kernel[offset]
    return result

def linear_pair(before_pair, after_pair):
    return (before_pair[0] * after_pair[0], after_pair[0] * before_pair[1] + after_pair[1])

def rounded(values):
    return lax.optimization_barrier(values.astype(jnp.bfloat16)).astype(jnp.float32)

def group_sum(activations, weights, groups):
    group_width = activations.shape[1] // groups
    running = jnp.zeros((activations.shape[0], weights.shape[1]), jnp.float32)
    for group_index in range(groups):
        lower = group_index * group_width
        running = running + rounded(jnp.dot(activations[:, lower:lower + group_width], weights[lower:lower + group_width], preferred_element_type=jnp.float32))
    return running

def reference(residual, mix_input, gate_input, mix_kernel, recur_gate_map, input_gate_map, decay_param, jump_log, out_weight, mix_gain, inner_gain, final_gain, gate_weight, value_weight, gate_kernel, value_kernel, down_weight):
    length = mix_input.shape[0]
    padded = jnp.pad(mix_input.astype(jnp.float32), ((MIX_TAPS - 1, 0), (0, 0)))
    conv_rows = causal_taps(padded, mix_kernel, length).astype(jnp.bfloat16)
    grouped = conv_rows.astype(jnp.float32).reshape(length, NB, BW)
    recur_gate = jax.nn.sigmoid(jnp.einsum('tnd,nde->tne', grouped, recur_gate_map.astype(jnp.float32))).reshape(length, D)
    input_gate = jax.nn.sigmoid(jnp.einsum('tnd,nde->tne', grouped, input_gate_map.astype(jnp.float32))).reshape(length, D)
    log_decay = -GATE_SCALE * recur_gate * jax.nn.softplus(-decay_param) + jump_log
    drive = jnp.sqrt(-jnp.expm1(2.0 * log_decay)) * input_gate * conv_rows.astype(jnp.float32)
    ignored, state = lax.associative_scan(linear_pair, (jnp.exp(log_decay), drive), axis=0)
    branch = (state * jax.nn.gelu(gate_input.astype(jnp.float32), approximate=True)).astype(jnp.bfloat16)
    mixed = group_sum(branch, out_weight, N_TP).astype(jnp.bfloat16)
    hidden_state = (residual.astype(jnp.float32) + norm_scale(mixed, mix_gain)).astype(jnp.bfloat16)
    normed = norm_scale(hidden_state, inner_gain).astype(jnp.bfloat16)
    up_gate = jnp.dot(normed, gate_weight, preferred_element_type=jnp.float32).astype(jnp.bfloat16)
    up_value = jnp.dot(normed, value_weight, preferred_element_type=jnp.float32).astype(jnp.bfloat16)
    gate_conv = causal_taps(jnp.pad(up_gate.astype(jnp.float32), ((HIDDEN_TAPS - 1, 0), (0, 0))), gate_kernel, length)
    value_conv = causal_taps(jnp.pad(up_value.astype(jnp.float32), ((HIDDEN_TAPS - 1, 0), (0, 0))), value_kernel, length)
    activation = (jax.nn.gelu(gate_conv, approximate=True) * value_conv).astype(jnp.bfloat16)
    down = group_sum(activation, down_weight, N_TP).astype(jnp.bfloat16)
    return (hidden_state.astype(jnp.float32) + norm_scale(down, final_gain)).astype(jnp.bfloat16)
```

```python
import functools

import jax
import jax.numpy as jnp
from jax import lax
from jax.experimental import pallas as pl
from jax.experimental.pallas import tpu as pltpu
from jax.sharding import PartitionSpec as P

EPS = 1e-06
GATE_SCALE = 8.0
SEGMENTS = 8
LANES = 128
GELU_A = 0.7978845608028654
GELU_B = 0.044715


def gelu(v):
    return 0.5 * v * (1.0 + jnp.tanh(GELU_A * (v + GELU_B * (v * v * v))))


def minus_expm1(y):
    series = 1.0 + y * (1.0 / 7.0)
    for n in (6.0, 5.0, 4.0, 3.0, 2.0):
        series = 1.0 + y * (1.0 / n) * series
    return jnp.where(y > -0.3, -y * series, 1.0 - jnp.exp(y))


def sigmoid(v):
    return 0.5 * jnp.tanh(0.5 * v) + 0.5


def scan_kernel(
    x_ref, edge_ref, taps_ref, rmap_ref, imap_ref, soft_ref, jump_ref,
    cum_ref, loc_ref, seg_ref, ends_ref,
    xs, decay, drive,
):
    group = pl.program_id(0)
    groups = pl.num_programs(0)
    length = x_ref.shape[0]
    taps = taps_ref.shape[0]
    xs[0:8, :] = edge_ref[...].astype(jnp.float32)
    xs[8 : 8 + length, :] = x_ref[...].astype(jnp.float32)
    rows = length // 4
    kernel = taps_ref[...].astype(jnp.float32)
    soft = soft_ref[...]
    for at in range(0, length, rows):
        conv = jnp.zeros((rows, LANES), jnp.float32)
        for k in range(taps):
            first = 8 + at - (taps - 1) + k
            conv = conv + xs[first : first + rows, :] * kernel[k : k + 1, :]
        conv = conv.astype(jnp.bfloat16)
        rgate = sigmoid(jnp.dot(conv, rmap_ref[0], preferred_element_type=jnp.float32))
        igate = sigmoid(jnp.dot(conv, imap_ref[0], preferred_element_type=jnp.float32))
        log_decay = -GATE_SCALE * rgate * soft + jump_ref[at : at + rows, :]
        decay[at : at + rows, :] = jnp.exp(log_decay)
        drive[at : at + rows, :] = (
            jnp.sqrt(minus_expm1(2.0 * log_decay)) * igate * conv.astype(jnp.float32)
        )
    steps = length // SEGMENTS

    def step(i, carry):
        state, product = carry
        where = pl.ds(i, SEGMENTS, steps)
        a = decay[where, :]
        state = a * state + drive[where, :]
        product = a * product
        loc_ref[where, :] = state
        cum_ref[where, :] = product
        return state, product

    zero = jnp.zeros((SEGMENTS, LANES), jnp.float32)
    state, product = lax.fori_loop(0, steps, step, (zero, zero + 1.0), unroll=8)
    seg_ref[0, :, :] = product
    seg_ref[1, :, :] = state
    all_state = state[0:1]
    all_product = product[0:1]
    for s in range(1, SEGMENTS):
        all_state = product[s : s + 1] * all_state + state[s : s + 1]
        all_product = product[s : s + 1] * all_product
    count = ends_ref.shape[0]
    ends_ref[:, pl.ds(group, 1), :] = jnp.broadcast_to(all_product[None], (count, 1, LANES))
    ends_ref[:, pl.ds(groups + group, 1), :] = jnp.broadcast_to(all_state[None], (count, 1, LANES))


def local_scan(x, edge, taps, rmap, imap, soft, jump, copies):
    length, channels = x.shape
    groups = channels // LANES
    column = lambda rows: pl.BlockSpec((rows, LANES), lambda g: (0, g))
    square = pl.BlockSpec((1, LANES, LANES), lambda g: (g, 0, 0))
    return pl.pallas_call(
        scan_kernel,
        grid=(groups,),
        in_specs=[column(length), column(8), column(taps.shape[0]), square, square, column(1), column(length)],
        out_specs=[
            column(length),
            column(length),
            pl.BlockSpec((2, SEGMENTS, LANES), lambda g: (0, 0, g)),
            pl.BlockSpec((copies, 2 * groups, LANES), lambda g: (0, 0, 0)),
        ],
        out_shape=[
            jax.ShapeDtypeStruct((length, channels), jnp.float32),
            jax.ShapeDtypeStruct((length, channels), jnp.float32),
            jax.ShapeDtypeStruct((2, SEGMENTS, channels), jnp.float32),
            jax.ShapeDtypeStruct((copies, 2 * groups, LANES), jnp.float32),
        ],
        scratch_shapes=[
            pltpu.VMEM((length + 8, LANES), jnp.float32),
            pltpu.VMEM((length, LANES), jnp.float32),
            pltpu.VMEM((length, LANES), jnp.float32),
        ],
        name="local_scan",
    )(x, edge, taps, rmap, imap, soft, jump)


def branch_kernel(me_ref, arrived_ref, seg_ref, cum_ref, loc_ref, gate_ref, w_ref, out_ref, carry, branch):
    block = pl.program_id(0)
    groups = cum_ref.shape[1] // LANES
    count = arrived_ref.shape[0]
    rows = cum_ref.shape[0]
    seg_rows = rows * pl.num_programs(0) // SEGMENTS
    per_block = rows // seg_rows

    @pl.when(block == 0)
    def _():
        def join(j, state):
            return arrived_ref[j, 0:groups, :] * state + arrived_ref[j, groups : 2 * groups, :]

        state = lax.fori_loop(0, me_ref[0], join, jnp.zeros((groups, LANES), jnp.float32))
        for g in range(groups):
            lanes = slice(g * LANES, (g + 1) * LANES)
            now = state[g : g + 1, :]
            for s in range(SEGMENTS):
                carry[s, 0:1, lanes] = now
                now = seg_ref[0, s : s + 1, lanes] * now + seg_ref[1, s : s + 1, lanes]

    for part in range(per_block):
        at = slice(part * seg_rows, (part + 1) * seg_rows)
        state = loc_ref[at, :] + cum_ref[at, :] * carry[block * per_block + part, 0:1, :]
        branch[at, :] = state
    gate = gate_ref[...].astype(jnp.float32)
    out = (branch[...] * gelu(gate)).astype(jnp.bfloat16)
    out_ref[0] = jnp.dot(out, w_ref[...], preferred_element_type=jnp.float32).astype(jnp.bfloat16)


def branch_shares(me, arrived, seg, cum, loc, gate, weight, blocks):
    length, channels = cum.shape
    width = weight.shape[1]
    rows = length // blocks
    row_block = pl.BlockSpec((rows, channels), lambda b: (b, 0))
    whole = lambda a: pl.BlockSpec(a.shape, lambda b: (0,) * a.ndim)
    return pl.pallas_call(
        branch_kernel,
        grid=(blocks,),
        in_specs=[
            pl.BlockSpec(memory_space=pltpu.SMEM),
            whole(arrived), whole(seg), row_block, row_block, row_block, whole(weight),
        ],
        out_specs=pl.BlockSpec((1, rows, width), lambda b: (b, 0, 0)),
        out_shape=jax.ShapeDtypeStruct((blocks, rows, width), jnp.bfloat16),
        scratch_shapes=[
            pltpu.VMEM((SEGMENTS, 1, channels), jnp.float32),
            pltpu.VMEM((rows, channels), jnp.float32),
        ],
        name="branch_shares",
    )(me, arrived, seg, cum, loc, gate, weight)


def scaled(v, gain):
    return v * lax.rsqrt(jnp.mean(v * v, axis=-1, keepdims=True) + EPS) * gain


def arrived_sum(ref):
    total = ref[0].astype(jnp.float32)
    for k in range(1, ref.shape[0]):
        total = total + ref[k].astype(jnp.float32)
    return total.astype(jnp.bfloat16).astype(jnp.float32)


def mid_kernel(me_ref, shares_ref, res_ref, mix_ref, inner_ref, hidden_ref, normed_ref):
    hidden = (
        res_ref[...].astype(jnp.float32) + scaled(arrived_sum(shares_ref), mix_ref[...])
    ).astype(jnp.bfloat16)
    hidden_ref[...] = hidden
    normed_ref[...] = scaled(hidden.astype(jnp.float32), inner_ref[...]).astype(jnp.bfloat16)


def mid(me, shares, residual, mix_gain, inner_gain):
    count, rows, width = shares.shape
    gain = pl.BlockSpec((1, width), lambda i, me: (0, 0))
    steps = 1
    some = pl.BlockSpec((rows // steps, width), lambda i, me: (i, 0))
    return pl.pallas_call(
        mid_kernel,
        grid_spec=pltpu.PrefetchScalarGridSpec(
            num_scalar_prefetch=1,
            grid=(steps,),
            in_specs=[
                pl.BlockSpec((count, rows // steps, width), lambda i, me: (0, i, 0)),
                pl.BlockSpec((rows // steps, width), lambda i, me: (me[0] * steps + i, 0)),
                gain,
                gain,
            ],
            out_specs=[some, some],
        ),
        out_shape=[jax.ShapeDtypeStruct((rows, width), jnp.bfloat16)] * 2,
        name="mid",
    )(me, shares, residual, mix_gain, inner_gain)


def last_kernel(shares_ref, hidden_ref, gain_ref, out_ref):
    out_ref[...] = (
        hidden_ref[...].astype(jnp.float32) + scaled(arrived_sum(shares_ref), gain_ref[...])
    ).astype(jnp.bfloat16)


def last(shares, hidden, gain):
    return pl.pallas_call(
        last_kernel,
        out_shape=jax.ShapeDtypeStruct(hidden.shape, jnp.bfloat16),
        name="last",
    )(shares, hidden, gain)


def from_behind(value, axis):
    count = lax.axis_size(axis)
    return lax.ppermute(value, axis, [(i, i + 1) for i in range(count - 1)])


def exchanged(tiles, axis):
    return lax.all_to_all(tiles, axis, split_axis=0, concat_axis=0, tiled=True)


def causal_taps(padded, kernel, length):
    kernel = kernel.astype(jnp.float32)
    result = jnp.zeros((length, padded.shape[1]), jnp.float32)
    for offset in range(kernel.shape[0]):
        result = result + padded[offset : offset + length] * kernel[offset]
    return result


def local(
    residual,
    mix_input,
    gate_input,
    mix_kernel,
    recur_gate_map,
    input_gate_map,
    decay_param,
    jump_log,
    out_weight,
    mix_gain,
    inner_gain,
    final_gain,
    gate_weight,
    value_weight,
    gate_kernel,
    value_kernel,
    down_weight,
):
    length = mix_input.shape[0]
    n_tp, n_sp = lax.axis_size("tp"), lax.axis_size("sp")
    tp_me = lax.axis_index("tp").astype(jnp.int32).reshape(1)
    sp_me = lax.axis_index("sp").astype(jnp.int32).reshape(1)
    hidden_units = gate_weight.shape[1]

    edge = from_behind(mix_input[length - 8 :], "sp")
    up_whole = lax.all_gather(
        jnp.concatenate([gate_weight, value_weight], axis=1), "sp", axis=0, tiled=True
    )
    turned = lax.optimization_barrier((down_weight.T, edge))[0]
    down_whole = lax.all_gather(turned, "sp", axis=0, tiled=True)

    soft = jax.nn.softplus(-decay_param)[None]
    cum, loc, seg, ends = local_scan(
        mix_input, edge, mix_kernel, recur_gate_map, input_gate_map, soft, jump_log, n_sp
    )
    arrived = exchanged(ends, "sp")
    shares = branch_shares(sp_me, arrived, seg, cum, loc, gate_input, out_weight, n_tp)
    hidden_state, normed = mid(
        tp_me, exchanged(shares, "tp"), residual, mix_gain[None], inner_gain[None]
    )
    everyone = exchanged(jnp.broadcast_to(normed, (n_tp, *normed.shape)), "tp").reshape(length, -1)

    up_gate = jnp.dot(
        everyone, up_whole[:, :hidden_units], preferred_element_type=jnp.float32
    ).astype(jnp.bfloat16)
    up_value = jnp.dot(
        everyone, up_whole[:, hidden_units:], preferred_element_type=jnp.float32
    ).astype(jnp.bfloat16)
    behind = gate_kernel.shape[0] - 1
    tails = jnp.stack([up_gate[length - behind :], up_value[length - behind :]])
    hidden_edge = from_behind(tails, "sp")
    gate_conv = causal_taps(
        jnp.concatenate([hidden_edge[0], up_gate], axis=0).astype(jnp.float32), gate_kernel, length
    )
    value_conv = causal_taps(
        jnp.concatenate([hidden_edge[1], up_value], axis=0).astype(jnp.float32), value_kernel, length
    )
    activation = (jax.nn.gelu(gate_conv, approximate=True) * value_conv).astype(jnp.bfloat16)
    down = lax.dot_general(
        activation, down_whole, (((1,), (1,)), ((), ())), preferred_element_type=jnp.float32
    ).astype(jnp.bfloat16)
    down_shares = exchanged(down.reshape(n_tp, length // n_tp, -1), "tp")
    return last(down_shares, hidden_state, final_gain[None])


def solution(mesh):
    return jax.shard_map(
        local,
        mesh=mesh,
        in_specs=(
            P(("grp", "sp"), None),
            P(("grp", "sp"), "tp"),
            P(("grp", "sp"), "tp"),
            P(None, "tp"),
            P("tp", None, None),
            P("tp", None, None),
            P("tp"),
            P(("grp", "sp"), "tp"),
            P("tp", None),
            P(),
            P(),
            P(),
            P("sp", "tp"),
            P("sp", "tp"),
            P(None, "tp"),
            P(None, "tp"),
            P("tp", "sp"),
        ),
        out_specs=P(("grp", "sp", "tp"), None),
        check_vma=False,
    )
```

```python
import functools

import jax
import jax.numpy as jnp
from jax import lax
from jax.experimental import pallas as pl
from jax.experimental.pallas import tpu as pltpu
from jax.sharding import PartitionSpec as P

EPS = 1e-06
GATE_SCALE = 8.0
SEGMENTS = 8
LANES = 128
BLOCKS = 4
HALO = 16
GELU_A = 0.7978845608028654
GELU_B = 0.044715


def gelu(v):
    return 0.5 * v * (1.0 + jnp.tanh(GELU_A * (v + GELU_B * (v * v * v))))


def minus_expm1(y):
    series = 1.0 + y * (1.0 / 7.0)
    for n in (6.0, 5.0, 4.0, 3.0, 2.0):
        series = 1.0 + y * (1.0 / n) * series
    return jnp.where(y > -0.3, -y * series, 1.0 - jnp.exp(y))


def sigmoid(v):
    return 0.5 * jnp.tanh(0.5 * v) + 0.5


def scan_kernel(
    x_ref, edge_ref, taps_ref, rmap_ref, imap_ref, soft_ref, jump_ref,
    cum_ref, loc_ref, seg_ref, ends_ref,
    xs, decay, drive,
):
    group = pl.program_id(0)
    groups = pl.num_programs(0)
    length = x_ref.shape[0]
    taps = taps_ref.shape[0]
    xs[0:8, :] = edge_ref[...].astype(jnp.float32)
    xs[8 : 8 + length, :] = x_ref[...].astype(jnp.float32)
    rows = length // 4
    kernel = taps_ref[...].astype(jnp.float32)
    v = -soft_ref[...]
    soft = jnp.maximum(v, 0.0) + jnp.log1p(jnp.exp(-jnp.abs(v)))
    for at in range(0, length, rows):
        conv = jnp.zeros((rows, LANES), jnp.float32)
        for k in range(taps):
            first = 8 + at - (taps - 1) + k
            conv = conv + xs[first : first + rows, :] * kernel[k : k + 1, :]
        conv = conv.astype(jnp.bfloat16)
        rgate = sigmoid(jnp.dot(conv, rmap_ref[0], preferred_element_type=jnp.float32))
        igate = sigmoid(jnp.dot(conv, imap_ref[0], preferred_element_type=jnp.float32))
        log_decay = -GATE_SCALE * rgate * soft + jump_ref[at : at + rows, :]
        decay[at : at + rows, :] = jnp.exp(log_decay)
        drive[at : at + rows, :] = (
            jnp.sqrt(minus_expm1(2.0 * log_decay)) * igate * conv.astype(jnp.float32)
        )
    steps = length // SEGMENTS

    def step(i, carry):
        state, product = carry
        where = pl.ds(i, SEGMENTS, steps)
        a = decay[where, :]
        state = a * state + drive[where, :]
        product = a * product
        loc_ref[where, :] = state
        cum_ref[where, :] = product
        return state, product

    zero = jnp.zeros((SEGMENTS, LANES), jnp.float32)
    state, product = lax.fori_loop(0, steps, step, (zero, zero + 1.0), unroll=8)
    seg_ref[0, :, :] = product
    seg_ref[1, :, :] = state
    all_state = state[0:1]
    all_product = product[0:1]
    for s in range(1, SEGMENTS):
        all_state = product[s : s + 1] * all_state + state[s : s + 1]
        all_product = product[s : s + 1] * all_product
    count = ends_ref.shape[0]
    ends_ref[:, pl.ds(group, 1), :] = jnp.broadcast_to(all_product[None], (count, 1, LANES))
    ends_ref[:, pl.ds(groups + group, 1), :] = jnp.broadcast_to(all_state[None], (count, 1, LANES))


def local_scan(x, edge, taps, rmap, imap, soft, jump, copies):
    length, channels = x.shape
    groups = channels // LANES
    column = lambda rows: pl.BlockSpec((rows, LANES), lambda g: (0, g))
    square = pl.BlockSpec((1, LANES, LANES), lambda g: (g, 0, 0))
    return pl.pallas_call(
        scan_kernel,
        grid=(groups,),
        in_specs=[column(length), column(8), column(taps.shape[0]), square, square, column(1), column(length)],
        out_specs=[
            column(length),
            column(length),
            pl.BlockSpec((2, SEGMENTS, LANES), lambda g: (0, 0, g)),
            pl.BlockSpec((copies, 2 * groups, LANES), lambda g: (0, 0, 0)),
        ],
        out_shape=[
            jax.ShapeDtypeStruct((length, channels), jnp.float32),
            jax.ShapeDtypeStruct((length, channels), jnp.float32),
            jax.ShapeDtypeStruct((2, SEGMENTS, channels), jnp.float32),
            jax.ShapeDtypeStruct((copies, 2 * groups, LANES), jnp.float32),
        ],
        scratch_shapes=[
            pltpu.VMEM((length + 8, LANES), jnp.float32),
            pltpu.VMEM((length, LANES), jnp.float32),
            pltpu.VMEM((length, LANES), jnp.float32),
        ],
        name="local_scan",
    )(x, edge, taps, rmap, imap, soft, jump)


def branch_kernel(me_ref, arrived_ref, seg_ref, cum_ref, loc_ref, gate_ref, w_ref, *rest):
    outs, carry, branch = rest[:-2], rest[-2], rest[-1]
    block = row_block_at(pl.program_id(0), me_ref, len(outs) == 2)
    groups = cum_ref.shape[1] // LANES
    rows = cum_ref.shape[0]
    per_block = SEGMENTS // BLOCKS
    seg_rows = rows // per_block

    @pl.when(pl.program_id(0) == 0)
    def _():
        def join(j, state):
            return arrived_ref[j, 0:groups, :] * state + arrived_ref[j, groups : 2 * groups, :]

        state = lax.fori_loop(0, me_ref[1], join, jnp.zeros((groups, LANES), jnp.float32))
        for g in range(groups):
            lanes = slice(g * LANES, (g + 1) * LANES)
            now = state[g : g + 1, :]
            for s in range(SEGMENTS):
                carry[s, 0:1, lanes] = now
                now = seg_ref[0, s : s + 1, lanes] * now + seg_ref[1, s : s + 1, lanes]

    for part in range(per_block):
        at = slice(part * seg_rows, (part + 1) * seg_rows)
        state = loc_ref[at, :] + cum_ref[at, :] * carry[block * per_block + part, 0:1, :]
        branch[at, :] = state
    gate = gate_ref[...].astype(jnp.float32)
    out = (branch[...] * gelu(gate)).astype(jnp.bfloat16)
    share = jnp.dot(out, w_ref[...], preferred_element_type=jnp.float32).astype(jnp.bfloat16)
    put(outs, share)


def row_block_at(step, me_ref, opposite):
    turned = 2 if opposite else 1 + (step * (5 - step) >> 1)
    return lax.rem(me_ref[0] + turned, BLOCKS)


def put(outs, share):
    if len(outs) == 1:
        outs[0][0] = share
    else:
        half = share.shape[1] // 2
        outs[0][...] = share[:, :half]
        outs[1][...] = share[:, half:]


def share_outputs(count, rows, width, halves):
    if halves:
        return (
            [pl.BlockSpec((rows, width // 2), lambda b, *_: (0, 0))] * 2,
            [jax.ShapeDtypeStruct((rows, width // 2), jnp.bfloat16)] * 2,
        )
    return (
        [pl.BlockSpec((1, rows, width), lambda b, *_: (b, 0, 0))],
        [jax.ShapeDtypeStruct((count, rows, width), jnp.bfloat16)],
    )


def branch_shares(me, arrived, seg, cum, loc, gate, weight, halves):
    length, channels = cum.shape
    width = weight.shape[1]
    rows = length // BLOCKS
    count = 1 if halves else BLOCKS - 1
    row_block = pl.BlockSpec((rows, channels), lambda b, me: (row_block_at(b, me, halves), 0))
    whole = lambda a: pl.BlockSpec(a.shape, lambda b, me: (0,) * a.ndim)
    out_specs, out_shape = share_outputs(count, rows, width, halves)
    return pl.pallas_call(
        branch_kernel,
        grid_spec=pltpu.PrefetchScalarGridSpec(
            num_scalar_prefetch=1,
            grid=(count,),
            in_specs=[whole(arrived), whole(seg), row_block, row_block, row_block, whole(weight)],
            out_specs=out_specs,
            scratch_shapes=[
                pltpu.VMEM((SEGMENTS, 1, channels), jnp.float32),
                pltpu.VMEM((rows, channels), jnp.float32),
            ],
        ),
        out_shape=out_shape,
        cost_estimate=pl.CostEstimate(
            flops=2 * count * rows * channels * width,
            bytes_accessed=count * rows * (10 * channels + 2 * width) + 2 * channels * width,
            transcendentals=count * rows * channels,
        ),
        name="branch_first" if halves else "branch_rest",
    )(me, arrived, seg, cum, loc, gate, weight)


def feed_kernel(*refs, names, first):
    me_ref, outside, own, right, left, low, high, w_ref, w_all, gk_ref, vk_ref = refs[:11]
    outs = refs[11:-5]
    lhs, up, act, down, sem = refs[-5:]
    chunk = pl.program_id(0)
    rows = own.shape[0]
    tall = rows + HALO
    taps = gk_ref.shape[0]
    width, units = down.shape
    half = width // 2
    fetch = pltpu.make_async_copy(w_all.at[:, pl.ds(2 * units, units)], down, sem)

    def fill(b, name):
        at = b * tall
        tail = slice(rows - HALO, rows)
        steps = {"own": 0, "right": 1, "opposite": 2, "left": 3}[name]
        if name == "left":
            lhs[at : at + HALO, :half] = low[tail, :]
            lhs[at : at + HALO, half:] = high[tail, :]
        else:
            behind = {"own": left, "right": own, "opposite": right}[name]
            lhs[at : at + HALO, :] = behind[tail, :]

        @pl.when(lax.rem(me_ref[0] + steps, BLOCKS) == 0)
        def _():
            lhs[at : at + HALO, :] = outside[...]

        at = at + HALO
        if name == "opposite":
            lhs[at : at + rows, :half] = low[...]
            lhs[at : at + rows, half:] = high[...]
        else:
            lhs[at : at + rows, :] = {"own": own, "right": right, "left": left}[name][...]

    @pl.when(chunk == 0)
    def _():
        fetch.start()
        for b, name in enumerate(names):
            fill(b, name)

    up[...] = (
        jnp.dot(lhs[...], w_ref[...], preferred_element_type=jnp.float32)
        .astype(jnp.bfloat16)
        .astype(jnp.float32)
    )
    gate_taps = gk_ref[...].astype(jnp.float32)
    value_taps = vk_ref[...].astype(jnp.float32)
    lanes = pl.ds(pl.multiple_of(chunk * LANES, LANES), LANES)
    for b in range(len(names)):
        gate = jnp.zeros((rows, LANES), jnp.float32)
        value = jnp.zeros((rows, LANES), jnp.float32)
        for k in range(taps):
            at = b * tall + HALO - (taps - 1) + k
            gate = gate + up[at : at + rows, 0:LANES] * gate_taps[k : k + 1, :]
            value = value + up[at : at + rows, LANES : 2 * LANES] * value_taps[k : k + 1, :]
        act[b * rows : (b + 1) * rows, lanes] = (gelu(gate) * value).astype(jnp.bfloat16)

    @pl.when(chunk == pl.num_programs(0) - 1)
    def _():
        fetch.wait()
        for b in range(len(names)):
            share = lax.dot_general(
                act[b * rows : (b + 1) * rows, :],
                down[...],
                (((1,), (1,)), ((), ())),
                preferred_element_type=jnp.float32,
            ).astype(jnp.bfloat16)
            if first:
                put(outs, share)
            else:
                outs[0][b] = share


def feed(me, outside, blocks, weights, gate_kernel, value_kernel, names, first):
    count = len(names)
    rows, width = blocks[0].shape
    units = gate_kernel.shape[1]
    chunks = units // LANES
    taps = gate_kernel.shape[0]
    out_specs, out_shape = share_outputs(count, rows, width, first)
    if not first:
        out_specs = [pl.BlockSpec((count, rows, width), lambda c: (0, 0, 0))]
    return pl.pallas_call(
        functools.partial(feed_kernel, names=names, first=first),
        grid=(chunks,),
        in_specs=[
            pl.BlockSpec(memory_space=pltpu.SMEM),
            *[pl.BlockSpec(memory_space=pltpu.VMEM)] * (1 + len(blocks)),
            pl.BlockSpec((width, 2 * LANES), lambda c: (0, c)),
            pl.BlockSpec(memory_space=pl.ANY),
            pl.BlockSpec((taps, LANES), lambda c: (0, c)),
            pl.BlockSpec((taps, LANES), lambda c: (0, c)),
        ],
        out_specs=out_specs,
        out_shape=out_shape,
        scratch_shapes=[
            pltpu.VMEM((count * (rows + HALO), width), jnp.bfloat16),
            pltpu.VMEM((count * (rows + HALO), 2 * LANES), jnp.float32),
            pltpu.VMEM((count * rows, units), jnp.bfloat16),
            pltpu.VMEM((width, units), jnp.bfloat16),
            pltpu.SemaphoreType.DMA,
        ],
        cost_estimate=pl.CostEstimate(
            flops=6 * count * rows * width * units,
            bytes_accessed=6 * width * units + 4 * count * rows * width,
            transcendentals=count * rows * units,
        ),
        name="feed_first" if first else "feed_rest",
    )(me, outside, *blocks, weights, weights, gate_kernel, value_kernel)


def pack_kernel(gate_ref, value_ref, turned_ref, out_ref):
    units = gate_ref.shape[1]
    for at in range(0, units, LANES):
        out_ref[:, 2 * at : 2 * at + LANES] = gate_ref[:, at : at + LANES]
        out_ref[:, 2 * at + LANES : 2 * at + 2 * LANES] = value_ref[:, at : at + LANES]
    out_ref[:, 2 * units :] = turned_ref[...]


def packed(gate, value, turned):
    rows, units = gate.shape
    return pl.pallas_call(
        pack_kernel,
        out_shape=jax.ShapeDtypeStruct((rows, 3 * units), jnp.bfloat16),
        name="pack",
    )(gate, value, turned)


def scaled(v, gain):
    return v * lax.rsqrt(jnp.mean(v * v, axis=-1, keepdims=True) + EPS) * gain


def three_sum(rest_ref, left_ref, right_ref, at):
    total = rest_ref[2, at, :].astype(jnp.float32) + left_ref[at, :].astype(jnp.float32)
    total = total + right_ref[at, :].astype(jnp.float32)
    return total.astype(jnp.bfloat16).astype(jnp.float32)


def by_rows(rows, body):
    def step(i, carry):
        body(pl.ds(pl.multiple_of(i * HALO, HALO), HALO))
        return carry

    lax.fori_loop(0, rows // HALO, step, 0)


def mid_kernel(
    me_ref, rest_ref, left_ref, right_ref, res_ref, mix_ref, inner_ref,
    hidden_ref, normed_ref, res, sem,
):
    rows = left_ref.shape[0]
    first = pl.multiple_of(me_ref[0] * rows, rows)
    fetch = pltpu.make_async_copy(res_ref.at[pl.ds(first, rows), :], res, sem)
    fetch.start()
    mix, inner = mix_ref[...], inner_ref[...]
    fetch.wait()

    def body(at):
        hidden = (
            res[at, :].astype(jnp.float32)
            + scaled(three_sum(rest_ref, left_ref, right_ref, at), mix)
        ).astype(jnp.bfloat16)
        hidden_ref[at, :] = hidden
        normed_ref[at, :] = scaled(hidden.astype(jnp.float32), inner).astype(jnp.bfloat16)

    by_rows(rows, body)


VMEM = pl.BlockSpec(memory_space=pltpu.VMEM)


def mid(me, rest, left, right, residual, mix_gain, inner_gain):
    rows, width = left.shape
    return pl.pallas_call(
        mid_kernel,
        in_specs=[
            pl.BlockSpec(memory_space=pltpu.SMEM),
            VMEM, VMEM, VMEM,
            pl.BlockSpec(memory_space=pl.ANY),
            VMEM, VMEM,
        ],
        out_specs=[VMEM, VMEM],
        out_shape=[jax.ShapeDtypeStruct((rows, width), jnp.bfloat16)] * 2,
        scratch_shapes=[pltpu.VMEM((rows, width), jnp.bfloat16), pltpu.SemaphoreType.DMA],
        name="mid",
    )(me, rest, left, right, residual, mix_gain, inner_gain)


def last_kernel(rest_ref, left_ref, right_ref, hidden_ref, gain_ref, out_ref):
    gain = gain_ref[...]

    def body(at):
        out_ref[at, :] = (
            hidden_ref[at, :].astype(jnp.float32)
            + scaled(three_sum(rest_ref, left_ref, right_ref, at), gain)
        ).astype(jnp.bfloat16)

    by_rows(hidden_ref.shape[0], body)


def last(rest, left, right, hidden, gain):
    return pl.pallas_call(
        last_kernel,
        in_specs=[VMEM] * 5,
        out_specs=VMEM,
        out_shape=jax.ShapeDtypeStruct(hidden.shape, jnp.bfloat16),
        name="last",
    )(rest, left, right, hidden, gain)


def join_kernel(rest_ref, low_ref, high_ref, right_ref, left_ref):
    half = low_ref.shape[1]
    add = lambda a, b: (a.astype(jnp.float32) + b.astype(jnp.float32)).astype(jnp.bfloat16)

    def body(at):
        right_ref[at, :half] = add(rest_ref[0, at, :half], low_ref[at, :])
        right_ref[at, half:] = rest_ref[0, at, half:]
        left_ref[at, :half] = rest_ref[1, at, :half]
        left_ref[at, half:] = add(rest_ref[1, at, half:], high_ref[at, :])

    by_rows(low_ref.shape[0], body)


def join(rest, low, high):
    _, rows, width = rest.shape
    return pl.pallas_call(
        join_kernel,
        in_specs=[VMEM] * 3,
        out_specs=[VMEM] * 2,
        out_shape=[jax.ShapeDtypeStruct((rows, width), jnp.bfloat16)] * 2,
        name="join",
    )(rest, low, high)


def turn(value, axis, steps):
    count = lax.axis_size(axis)
    return lax.ppermute(value, axis, [(i, (i + steps) % count) for i in range(count)])


def ring_sum(first, rest):
    low, high = turn(first[0], "tp", 1), turn(first[1], "tp", -1)
    to_right, to_left = join(rest, low, high)
    return rest, turn(to_right, "tp", 1), turn(to_left, "tp", -1)


def from_behind(value, axis):
    count = lax.axis_size(axis)
    return lax.ppermute(value, axis, [(i, i + 1) for i in range(count - 1)])


def exchanged(tiles, axis):
    return lax.all_to_all(tiles, axis, split_axis=0, concat_axis=0, tiled=True)


def local(
    residual,
    mix_input,
    gate_input,
    mix_kernel,
    recur_gate_map,
    input_gate_map,
    decay_param,
    jump_log,
    out_weight,
    mix_gain,
    inner_gain,
    final_gain,
    gate_weight,
    value_weight,
    gate_kernel,
    value_kernel,
    down_weight,
):
    n_tp, n_sp = lax.axis_size("tp"), lax.axis_size("sp")
    assert n_tp == BLOCKS
    tp_me = lax.axis_index("tp").astype(jnp.int32)
    me = jnp.stack([tp_me, lax.axis_index("sp").astype(jnp.int32)])

    edge = from_behind(mix_input[mix_input.shape[0] - 8 :], "sp")
    weights = lax.all_gather(packed(gate_weight, value_weight, down_weight.T), "sp", axis=0, tiled=True)

    cum, loc, seg, ends = local_scan(
        mix_input, edge, mix_kernel, recur_gate_map, input_gate_map, decay_param[None], jump_log, n_sp
    )
    arrived = exchanged(ends, "sp")
    shares = functools.partial(
        branch_shares, arrived=arrived, seg=seg, cum=cum, loc=loc, gate=gate_input, weight=out_weight
    )
    first = shares(me, halves=True)
    rest = shares(me, halves=False)[0]
    hidden_state, own = mid(
        me, *ring_sum(first, rest), residual, mix_gain[None], inner_gain[None]
    )
    left, right = turn(own, "tp", 1), turn(own, "tp", -1)
    half = own.shape[1] // 2
    low, high = turn(left[:, :half], "tp", 1), turn(right[:, half:], "tp", -1)
    tails = [own[-HALO:], right[-HALO:], jnp.concatenate([low[-HALO:], high[-HALO:]], axis=1), left[-HALO:]]
    outside = from_behind(lax.select_n(n_tp - 1 - tp_me, *tails), "sp")
    blocks = (own, right, left, low, high)
    given = (me, outside, blocks, weights, gate_kernel, value_kernel)
    first = feed(*given, names=("opposite",), first=True)
    rest = feed(*given, names=("right", "left", "own"), first=False)[0]
    return last(*ring_sum(first, rest), hidden_state, final_gain[None])


def solution(mesh):
    return jax.shard_map(
        local,
        mesh=mesh,
        in_specs=(
            P(("grp", "sp"), None),
            P(("grp", "sp"), "tp"),
            P(("grp", "sp"), "tp"),
            P(None, "tp"),
            P("tp", None, None),
            P("tp", None, None),
            P("tp"),
            P(("grp", "sp"), "tp"),
            P("tp", None),
            P(),
            P(),
            P(),
            P("sp", "tp"),
            P("sp", "tp"),
            P(None, "tp"),
            P(None, "tp"),
            P("tp", "sp"),
        ),
        out_specs=P(("grp", "sp", "tp"), None),
        check_vma=False,
    )
```

```python
import functools

import jax
import jax.numpy as jnp
from jax import lax
from jax.experimental import pallas as pl
from jax.experimental.pallas import tpu as pltpu
from jax.sharding import PartitionSpec as P

EPS = 1e-06
GATE_SCALE = 8.0
SEGMENTS = 8
LANES = 128
BLOCKS = 4
HALO = 16
MIB = 1 << 20
GELU_A = 0.7978845608028654
GELU_B = 0.044715


def gelu(v):
    return 0.5 * v * (1.0 + jnp.tanh(GELU_A * (v + GELU_B * (v * v * v))))


def minus_expm1(y):
    series = 1.0 + y * (1.0 / 7.0)
    for n in (6.0, 5.0, 4.0, 3.0, 2.0):
        series = 1.0 + y * (1.0 / n) * series
    return jnp.where(y > -0.3, -y * series, 1.0 - jnp.exp(y))


def sigmoid(v):
    return 0.5 * jnp.tanh(0.5 * v) + 0.5


def scan_kernel(
    x_ref, edge_ref, taps_ref, rmap_ref, imap_ref, soft_ref, jump_ref,
    cum_ref, loc_ref, seg_ref, ends_ref,
    xs, decay, drive,
):
    group = pl.program_id(0)
    groups = pl.num_programs(0)
    length = x_ref.shape[0]
    taps = taps_ref.shape[0]
    xs[0:8, :] = edge_ref[...].astype(jnp.float32)
    xs[8 : 8 + length, :] = x_ref[...].astype(jnp.float32)
    rows = length // 4
    kernel = taps_ref[...].astype(jnp.float32)
    v = -soft_ref[...]
    soft = jnp.maximum(v, 0.0) + jnp.log1p(jnp.exp(-jnp.abs(v)))
    for at in range(0, length, rows):
        conv = jnp.zeros((rows, LANES), jnp.float32)
        for k in range(taps):
            first = 8 + at - (taps - 1) + k
            conv = conv + xs[first : first + rows, :] * kernel[k : k + 1, :]
        conv = conv.astype(jnp.bfloat16)
        rgate = sigmoid(jnp.dot(conv, rmap_ref[0], preferred_element_type=jnp.float32))
        igate = sigmoid(jnp.dot(conv, imap_ref[0], preferred_element_type=jnp.float32))
        log_decay = -GATE_SCALE * rgate * soft + jump_ref[at : at + rows, :]
        decay[at : at + rows, :] = jnp.exp(log_decay)
        drive[at : at + rows, :] = (
            jnp.sqrt(minus_expm1(2.0 * log_decay)) * igate * conv.astype(jnp.float32)
        )
    steps = length // SEGMENTS

    def step(i, carry):
        state, product = carry
        where = pl.ds(i, SEGMENTS, steps)
        a = decay[where, :]
        state = a * state + drive[where, :]
        product = a * product
        loc_ref[where, :] = state
        cum_ref[where, :] = product
        return state, product

    zero = jnp.zeros((SEGMENTS, LANES), jnp.float32)
    state, product = lax.fori_loop(0, steps, step, (zero, zero + 1.0), unroll=8)
    seg_ref[0, :, :] = product
    seg_ref[1, :, :] = state
    all_state = state[0:1]
    all_product = product[0:1]
    for s in range(1, SEGMENTS):
        all_state = product[s : s + 1] * all_state + state[s : s + 1]
        all_product = product[s : s + 1] * all_product
    count = ends_ref.shape[0]
    ends_ref[:, pl.ds(group, 1), :] = jnp.broadcast_to(all_product[None], (count, 1, LANES))
    ends_ref[:, pl.ds(groups + group, 1), :] = jnp.broadcast_to(all_state[None], (count, 1, LANES))


def local_scan(x, edge, taps, rmap, imap, soft, jump, copies):
    length, channels = x.shape
    groups = channels // LANES
    column = lambda rows: pl.BlockSpec((rows, LANES), lambda g: (0, g))
    square = pl.BlockSpec((1, LANES, LANES), lambda g: (g, 0, 0))
    return pl.pallas_call(
        scan_kernel,
        grid=(groups,),
        in_specs=[column(length), column(8), column(taps.shape[0]), square, square, column(1), column(length)],
        out_specs=[
            column(length),
            column(length),
            pl.BlockSpec((2, SEGMENTS, LANES), lambda g: (0, 0, g)),
            pl.BlockSpec((copies, 2 * groups, LANES), lambda g: (0, 0, 0)),
        ],
        out_shape=[
            jax.ShapeDtypeStruct((length, channels), jnp.float32),
            jax.ShapeDtypeStruct((length, channels), jnp.float32),
            jax.ShapeDtypeStruct((2, SEGMENTS, channels), jnp.float32),
            jax.ShapeDtypeStruct((copies, 2 * groups, LANES), jnp.float32),
        ],
        scratch_shapes=[
            pltpu.VMEM((length + 8, LANES), jnp.float32),
            pltpu.VMEM((length, LANES), jnp.float32),
            pltpu.VMEM((length, LANES), jnp.float32),
        ],
        compiler_params=pltpu.CompilerParams(vmem_limit_bytes=12 * MIB),
        name="local_scan",
    )(x, edge, taps, rmap, imap, soft, jump)


def branch_kernel(me_ref, arrived_ref, seg_ref, cum_ref, loc_ref, gate_ref, w_ref, *rest):
    outs, carry, branch = rest[:-2], rest[-2], rest[-1]
    length, channels = cum_ref.shape
    groups = channels // LANES
    rows = length // BLOCKS
    per_block = SEGMENTS // BLOCKS
    seg_rows = rows // per_block

    def join(j, state):
        return arrived_ref[j, 0:groups, :] * state + arrived_ref[j, groups : 2 * groups, :]

    state = lax.fori_loop(0, me_ref[1], join, jnp.zeros((groups, LANES), jnp.float32))
    for g in range(groups):
        lanes = slice(g * LANES, (g + 1) * LANES)
        now = state[g : g + 1, :]
        for s in range(SEGMENTS):
            carry[s, 0:1, lanes] = now
            now = seg_ref[0, s : s + 1, lanes] * now + seg_ref[1, s : s + 1, lanes]

    for b, steps in enumerate((2,) if len(outs) == 2 else (1, 3, 0)):
        block = lax.rem(me_ref[0] + steps, BLOCKS)
        first = pl.multiple_of(block * rows, rows)
        for part in range(per_block):
            at = pl.ds(pl.multiple_of(first + part * seg_rows, 8), seg_rows)
            state = loc_ref[at, :] + cum_ref[at, :] * carry[block * per_block + part, 0:1, :]
            branch[part * seg_rows : (part + 1) * seg_rows, :] = state
        gate = gate_ref[pl.ds(first, rows), :].astype(jnp.float32)
        out = (branch[...] * gelu(gate)).astype(jnp.bfloat16)
        share = jnp.dot(out, w_ref[...], preferred_element_type=jnp.float32).astype(jnp.bfloat16)
        if len(outs) == 2:
            put(outs, share)
        else:
            outs[0][b] = share


def put(outs, share):
    half = share.shape[1] // 2
    outs[0][...] = share[:, :half]
    outs[1][...] = share[:, half:]


VMEM = pl.BlockSpec(memory_space=pltpu.VMEM)


def vm(value):
    return pltpu.with_memory_space_constraint(value, pltpu.VMEM)


def vm_out(shape):
    return pltpu.VMEM(shape, jnp.bfloat16)


def share_shapes(count, rows, width, halves):
    return [vm_out((rows, width // 2))] * 2 if halves else [vm_out((count, rows, width))]


def branch_shares(me, arrived, seg, cum, loc, gate, weight, halves):
    length, channels = cum.shape
    width = weight.shape[1]
    rows = length // BLOCKS
    count = 1 if halves else BLOCKS - 1
    out_shape = share_shapes(count, rows, width, halves)
    return pl.pallas_call(
        branch_kernel,
        in_specs=[pl.BlockSpec(memory_space=pltpu.SMEM), *[VMEM] * 6],
        out_specs=[VMEM] * len(out_shape),
        out_shape=out_shape,
        scratch_shapes=[
            pltpu.VMEM((SEGMENTS, 1, channels), jnp.float32),
            pltpu.VMEM((rows, channels), jnp.float32),
        ],
        cost_estimate=pl.CostEstimate(
            flops=2 * count * rows * channels * width,
            bytes_accessed=count * rows * (10 * channels + 2 * width) + 2 * channels * width,
            transcendentals=count * rows * channels,
        ),
        compiler_params=pltpu.CompilerParams(vmem_limit_bytes=20 * MIB),
        name="branch_first" if halves else "branch_rest",
    )(me, *map(vm, (arrived, seg, cum, loc)), gate, weight)


def feed_kernel(*refs, names, first):
    me_ref, outside, own, right, left, low, high, weights, gk_ref, vk_ref = refs[:10]
    outs = refs[10:-7]
    lhs, up_a, up_b, act, ring, down, sems = refs[-7:]
    rows = own.shape[0]
    tall = rows + HALO
    taps = gk_ref.shape[0]
    shards, chunks, shard_rows, _ = down.shape
    width = shards * shard_rows
    half = width // 2
    slots = ring.shape[0]
    get_down = pltpu.make_async_copy(weights.at[:, pl.ds(2 * chunks, chunks)], down, sems.at[slots])

    def get(chunk):
        slot = lax.rem(chunk, slots)
        return pltpu.make_async_copy(weights.at[:, pl.ds(2 * chunk, 2)], ring.at[slot], sems.at[slot])

    def fill(b, name):
        at = b * tall
        tail = slice(rows - HALO, rows)
        steps = {"own": 0, "right": 1, "opposite": 2, "left": 3}[name]
        if name == "left":
            lhs[at : at + HALO, :half] = low[tail, :]
            lhs[at : at + HALO, half:] = high[tail, :]
        else:
            behind = {"own": left, "right": own, "opposite": right}[name]
            lhs[at : at + HALO, :] = behind[tail, :]

        @pl.when(lax.rem(me_ref[0] + steps, BLOCKS) == 0)
        def _():
            lhs[at : at + HALO, :] = outside[...]

        at = at + HALO
        if name == "opposite":
            lhs[at : at + rows, :half] = low[...]
            lhs[at : at + rows, half:] = high[...]
        else:
            lhs[at : at + rows, :] = {"own": own, "right": right, "left": left}[name][...]

    def activate(chunk, up):
        lanes = pl.ds(pl.multiple_of(chunk * LANES, LANES), LANES)
        gate_taps = gk_ref[:, lanes].astype(jnp.float32)
        value_taps = vk_ref[:, lanes].astype(jnp.float32)
        for b in range(len(names)):
            gate = jnp.zeros((rows, LANES), jnp.float32)
            value = jnp.zeros((rows, LANES), jnp.float32)
            for k in range(taps):
                at = b * tall + HALO - (taps - 1) + k
                gate = gate + up[at : at + rows, 0:LANES] * gate_taps[k : k + 1, :]
                value = value + up[at : at + rows, LANES : 2 * LANES] * value_taps[k : k + 1, :]
            act[b * rows : (b + 1) * rows, lanes] = (gelu(gate) * value).astype(jnp.bfloat16)

    def project(chunk, up):
        slot = lax.rem(chunk, slots)
        sides = [ring[slot, :, side].reshape(width, LANES) for side in range(2)]
        up[...] = (
            jnp.dot(lhs[...], jnp.concatenate(sides, axis=1), preferred_element_type=jnp.float32)
            .astype(jnp.bfloat16)
            .astype(jnp.float32)
        )

    for chunk in range(slots - 1):
        get(jnp.int32(chunk)).start()
    get_down.start()
    for b, name in enumerate(names):
        fill(b, name)
    get(jnp.int32(0)).wait()
    project(jnp.int32(0), up_a)

    def ahead(chunk):
        @pl.when(chunk < chunks)
        def _():
            get(chunk).start()

    def pair(i, carry):
        chunk = 2 * i
        ahead(chunk + 3)
        ahead(chunk + 4)
        get(chunk + 1).wait()
        get(chunk + 2).wait()
        activate(chunk, up_a)
        project(chunk + 1, up_b)
        activate(chunk + 1, up_b)
        project(chunk + 2, up_a)
        return carry

    lax.fori_loop(0, chunks // 2, pair, 0)
    get_down.wait()
    activate(jnp.int32(chunks - 1), up_a)
    turned = jnp.concatenate([down[:, c].reshape(width, LANES) for c in range(chunks)], axis=1)
    share = lax.dot_general(
        act[...], turned, (((1,), (1,)), ((), ())), preferred_element_type=jnp.float32
    ).astype(jnp.bfloat16)
    if first:
        put(outs, share)
    else:
        for b in range(len(names)):
            outs[0][b] = share[b * rows : (b + 1) * rows, :]


def feed(me, outside, blocks, weights, gate_kernel, value_kernel, names, first):
    count = len(names)
    rows, width = blocks[0].shape
    units = gate_kernel.shape[1]
    assert units // LANES % 2 == 1
    shards, _, shard_rows, _ = weights.shape
    tall = count * (rows + HALO)
    out_shape = share_shapes(count, rows, width, first)
    return pl.pallas_call(
        functools.partial(feed_kernel, names=names, first=first),
        in_specs=[
            pl.BlockSpec(memory_space=pltpu.SMEM),
            *[VMEM] * (1 + len(blocks)),
            pl.BlockSpec(memory_space=pl.ANY),
            VMEM,
            VMEM,
        ],
        out_specs=[VMEM] * len(out_shape),
        out_shape=out_shape,
        scratch_shapes=[
            pltpu.VMEM((tall, width), jnp.bfloat16),
            pltpu.VMEM((tall, 2 * LANES), jnp.float32),
            pltpu.VMEM((tall, 2 * LANES), jnp.float32),
            pltpu.VMEM((count * rows, units), jnp.bfloat16),
            pltpu.VMEM((4, shards, 2, shard_rows, LANES), jnp.bfloat16),
            pltpu.VMEM((shards, units // LANES, shard_rows, LANES), jnp.bfloat16),
            pltpu.SemaphoreType.DMA((5,)),
        ],
        cost_estimate=pl.CostEstimate(
            flops=6 * count * rows * width * units,
            bytes_accessed=6 * width * units + 4 * count * rows * width,
            transcendentals=count * rows * units,
        ),
        compiler_params=pltpu.CompilerParams(vmem_limit_bytes=36 * MIB),
        name="feed_first" if first else "feed_rest",
    )(me, vm(outside), *map(vm, blocks), weights, gate_kernel, value_kernel)


def pack_kernel(gate_ref, value_ref, turned_ref, out_ref):
    chunks = gate_ref.shape[1] // LANES
    for c in range(chunks):
        lanes = slice(c * LANES, (c + 1) * LANES)
        out_ref[2 * c] = gate_ref[:, lanes]
        out_ref[2 * c + 1] = value_ref[:, lanes]
        out_ref[2 * chunks + c] = turned_ref[:, lanes]


def packed(gate, value, turned):
    rows, units = gate.shape
    return pl.pallas_call(
        pack_kernel,
        out_shape=jax.ShapeDtypeStruct((3 * units // LANES, rows, LANES), jnp.bfloat16),
        compiler_params=pltpu.CompilerParams(vmem_limit_bytes=8 * MIB),
        name="pack",
    )(gate, value, turned)


def scaled(v, gain):
    return v * lax.rsqrt(jnp.mean(v * v, axis=-1, keepdims=True) + EPS) * gain


def three_sum(rest_ref, left_ref, right_ref, at):
    total = rest_ref[2, at, :].astype(jnp.float32) + left_ref[at, :].astype(jnp.float32)
    total = total + right_ref[at, :].astype(jnp.float32)
    return total.astype(jnp.bfloat16).astype(jnp.float32)


def by_rows(rows, body):
    def step(i, carry):
        body(pl.ds(pl.multiple_of(i * HALO, HALO), HALO))
        return carry

    lax.fori_loop(0, rows // HALO, step, 0)


def mid_kernel(
    me_ref, rest_ref, left_ref, right_ref, res_ref, mix_ref, inner_ref,
    hidden_ref, normed_ref, res, sem,
):
    rows = left_ref.shape[0]
    first = pl.multiple_of(me_ref[0] * rows, rows)
    fetch = pltpu.make_async_copy(res_ref.at[pl.ds(first, rows), :], res, sem)
    fetch.start()
    mix, inner = mix_ref[...], inner_ref[...]
    fetch.wait()

    def body(at):
        hidden = (
            res[at, :].astype(jnp.float32)
            + scaled(three_sum(rest_ref, left_ref, right_ref, at), mix)
        ).astype(jnp.bfloat16)
        hidden_ref[at, :] = hidden
        normed_ref[at, :] = scaled(hidden.astype(jnp.float32), inner).astype(jnp.bfloat16)

    by_rows(rows, body)


def mid(me, rest, left, right, residual, mix_gain, inner_gain):
    rows, width = left.shape
    return pl.pallas_call(
        mid_kernel,
        in_specs=[
            pl.BlockSpec(memory_space=pltpu.SMEM),
            VMEM, VMEM, VMEM,
            pl.BlockSpec(memory_space=pl.ANY),
            VMEM, VMEM,
        ],
        out_specs=[VMEM, VMEM],
        out_shape=[vm_out((rows, width))] * 2,
        scratch_shapes=[pltpu.VMEM((rows, width), jnp.bfloat16), pltpu.SemaphoreType.DMA],
        compiler_params=pltpu.CompilerParams(vmem_limit_bytes=12 * MIB),
        name="mid",
    )(me, vm(rest), vm(left), vm(right), residual, mix_gain, inner_gain)


def last_kernel(rest_ref, left_ref, right_ref, hidden_ref, gain_ref, out_ref):
    gain = gain_ref[...]

    def body(at):
        out_ref[at, :] = (
            hidden_ref[at, :].astype(jnp.float32)
            + scaled(three_sum(rest_ref, left_ref, right_ref, at), gain)
        ).astype(jnp.bfloat16)

    by_rows(hidden_ref.shape[0], body)


def last(rest, left, right, hidden, gain):
    return pl.pallas_call(
        last_kernel,
        in_specs=[VMEM] * 5,
        out_specs=VMEM,
        out_shape=jax.ShapeDtypeStruct(hidden.shape, jnp.bfloat16),
        compiler_params=pltpu.CompilerParams(vmem_limit_bytes=12 * MIB),
        name="last",
    )(*map(vm, (rest, left, right, hidden)), gain)


def join_kernel(rest_ref, low_ref, high_ref, right_ref, left_ref):
    half = low_ref.shape[1]
    add = lambda a, b: (a.astype(jnp.float32) + b.astype(jnp.float32)).astype(jnp.bfloat16)

    def body(at):
        right_ref[at, :half] = add(rest_ref[0, at, :half], low_ref[at, :])
        right_ref[at, half:] = rest_ref[0, at, half:]
        left_ref[at, :half] = rest_ref[1, at, :half]
        left_ref[at, half:] = add(rest_ref[1, at, half:], high_ref[at, :])

    by_rows(low_ref.shape[0], body)


def join(rest, low, high):
    _, rows, width = rest.shape
    return pl.pallas_call(
        join_kernel,
        in_specs=[VMEM] * 3,
        out_specs=[VMEM] * 2,
        out_shape=[vm_out((rows, width))] * 2,
        compiler_params=pltpu.CompilerParams(vmem_limit_bytes=12 * MIB),
        name="join",
    )(*map(vm, (rest, low, high)))


def turn(value, axis, steps):
    count = lax.axis_size(axis)
    return lax.ppermute(value, axis, [(i, (i + steps) % count) for i in range(count)])


def ring_sum(first, rest):
    low, high = turn(first[0], "tp", 1), turn(first[1], "tp", -1)
    to_right, to_left = join(rest, low, high)
    return rest, turn(to_right, "tp", 1), turn(to_left, "tp", -1)


def from_behind(value, axis):
    count = lax.axis_size(axis)
    return lax.ppermute(value, axis, [(i, i + 1) for i in range(count - 1)])


def exchanged(tiles, axis):
    return lax.all_to_all(tiles, axis, split_axis=0, concat_axis=0, tiled=True)


def local(
    residual,
    mix_input,
    gate_input,
    mix_kernel,
    recur_gate_map,
    input_gate_map,
    decay_param,
    jump_log,
    out_weight,
    mix_gain,
    inner_gain,
    final_gain,
    gate_weight,
    value_weight,
    gate_kernel,
    value_kernel,
    down_weight,
):
    n_tp, n_sp = lax.axis_size("tp"), lax.axis_size("sp")
    assert n_tp == BLOCKS
    tp_me = lax.axis_index("tp").astype(jnp.int32)
    me = jnp.stack([tp_me, lax.axis_index("sp").astype(jnp.int32)])

    edge = from_behind(mix_input[mix_input.shape[0] - 8 :], "sp")
    shard = packed(gate_weight, value_weight, down_weight.T)
    weights = lax.all_gather(shard, "sp", axis=0, tiled=True).reshape(n_sp, *shard.shape)

    cum, loc, seg, ends = local_scan(
        mix_input, edge, mix_kernel, recur_gate_map, input_gate_map, decay_param[None], jump_log, n_sp
    )
    arrived = exchanged(ends, "sp")
    shares = functools.partial(
        branch_shares, arrived=arrived, seg=seg, cum=cum, loc=loc, gate=gate_input, weight=out_weight
    )
    first = shares(me, halves=True)
    rest = shares(me, halves=False)[0]
    hidden_state, own = mid(
        me, *ring_sum(first, rest), residual, mix_gain[None], inner_gain[None]
    )
    left, right = turn(own, "tp", 1), turn(own, "tp", -1)
    half = own.shape[1] // 2
    low, high = turn(left[:, :half], "tp", 1), turn(right[:, half:], "tp", -1)
    tails = [own[-HALO:], right[-HALO:], jnp.concatenate([low[-HALO:], high[-HALO:]], axis=1), left[-HALO:]]
    outside = from_behind(lax.select_n(n_tp - 1 - tp_me, *tails), "sp")
    blocks = (own, right, left, low, high)
    given = (me, outside, blocks, weights, gate_kernel, value_kernel)
    first = feed(*given, names=("opposite",), first=True)
    rest = feed(*given, names=("right", "left", "own"), first=False)[0]
    return last(*ring_sum(first, rest), hidden_state, final_gain[None])


def solution(mesh):
    return jax.shard_map(
        local,
        mesh=mesh,
        in_specs=(
            P(("grp", "sp"), None),
            P(("grp", "sp"), "tp"),
            P(("grp", "sp"), "tp"),
            P(None, "tp"),
            P("tp", None, None),
            P("tp", None, None),
            P("tp"),
            P(("grp", "sp"), "tp"),
            P("tp", None),
            P(),
            P(),
            P(),
            P("sp", "tp"),
            P("sp", "tp"),
            P(None, "tp"),
            P(None, "tp"),
            P("tp", "sp"),
        ),
        out_specs=P(("grp", "sp", "tp"), None),
        check_vma=False,
    )
```

```python
import functools

import jax
import jax.numpy as jnp
from jax import lax
from jax.experimental import pallas as pl
from jax.experimental.pallas import tpu as pltpu
from jax.sharding import PartitionSpec as P

EPS = 1e-06
GATE_SCALE = 8.0
SEGMENTS = 8
LANES = 128
BLOCKS = 4
HALO = 16
MIB = 1 << 20
GELU_A = 0.7978845608028654
GELU_B = 0.044715


def gelu(v):
    return 0.5 * v * (1.0 + jnp.tanh(GELU_A * (v + GELU_B * (v * v * v))))


def minus_expm1(y):
    series = 1.0 + y * (1.0 / 7.0)
    for n in (6.0, 5.0, 4.0, 3.0, 2.0):
        series = 1.0 + y * (1.0 / n) * series
    return jnp.where(y > -0.3, -y * series, 1.0 - jnp.exp(y))


def sigmoid(v):
    return 0.5 * jnp.tanh(0.5 * v) + 0.5


def scan_kernel(
    x_ref, edge_ref, taps_ref, rmap_ref, imap_ref, soft_ref, jump_ref,
    cum_ref, loc_ref, seg_ref, ends_ref,
    xs, decay, drive,
):
    group = pl.program_id(0)
    groups = pl.num_programs(0)
    length = x_ref.shape[0]
    taps = taps_ref.shape[0]
    xs[0:8, :] = edge_ref[...].astype(jnp.float32)
    xs[8 : 8 + length, :] = x_ref[...].astype(jnp.float32)
    rows = length // 4
    kernel = taps_ref[...].astype(jnp.float32)
    v = -soft_ref[...]
    soft = jnp.maximum(v, 0.0) + jnp.log1p(jnp.exp(-jnp.abs(v)))
    for at in range(0, length, rows):
        conv = jnp.zeros((rows, LANES), jnp.float32)
        for k in range(taps):
            first = 8 + at - (taps - 1) + k
            conv = conv + xs[first : first + rows, :] * kernel[k : k + 1, :]
        conv = conv.astype(jnp.bfloat16)
        rgate = sigmoid(jnp.dot(conv, rmap_ref[0], preferred_element_type=jnp.float32))
        igate = sigmoid(jnp.dot(conv, imap_ref[0], preferred_element_type=jnp.float32))
        log_decay = -GATE_SCALE * rgate * soft + jump_ref[at : at + rows, :]
        decay[at : at + rows, :] = jnp.exp(log_decay)
        drive[at : at + rows, :] = (
            jnp.sqrt(minus_expm1(2.0 * log_decay)) * igate * conv.astype(jnp.float32)
        )
    steps = length // SEGMENTS

    def step(i, carry):
        state, product = carry
        where = pl.ds(i, SEGMENTS, steps)
        a = decay[where, :]
        state = a * state + drive[where, :]
        product = a * product
        loc_ref[where, :] = state
        cum_ref[where, :] = product
        return state, product

    zero = jnp.zeros((SEGMENTS, LANES), jnp.float32)
    state, product = lax.fori_loop(0, steps, step, (zero, zero + 1.0), unroll=8)
    seg_ref[0, :, :] = product
    seg_ref[1, :, :] = state
    all_state = state[0:1]
    all_product = product[0:1]
    for s in range(1, SEGMENTS):
        all_state = product[s : s + 1] * all_state + state[s : s + 1]
        all_product = product[s : s + 1] * all_product
    count = ends_ref.shape[0]
    ends_ref[:, pl.ds(group, 1), :] = jnp.broadcast_to(all_product[None], (count, 1, LANES))
    ends_ref[:, pl.ds(groups + group, 1), :] = jnp.broadcast_to(all_state[None], (count, 1, LANES))


def local_scan(x, edge, taps, rmap, imap, soft, jump, copies):
    length, channels = x.shape
    groups = channels // LANES
    column = lambda rows: pl.BlockSpec((rows, LANES), lambda g: (0, g))
    square = pl.BlockSpec((1, LANES, LANES), lambda g: (g, 0, 0))
    return pl.pallas_call(
        scan_kernel,
        grid=(groups,),
        in_specs=[column(length), column(8), column(taps.shape[0]), square, square, column(1), column(length)],
        out_specs=[
            column(length),
            column(length),
            pl.BlockSpec((2, SEGMENTS, LANES), lambda g: (0, 0, g)),
            pl.BlockSpec((copies, 2 * groups, LANES), lambda g: (0, 0, 0)),
        ],
        out_shape=[
            jax.ShapeDtypeStruct((length, channels), jnp.float32),
            jax.ShapeDtypeStruct((length, channels), jnp.float32),
            jax.ShapeDtypeStruct((2, SEGMENTS, channels), jnp.float32),
            jax.ShapeDtypeStruct((copies, 2 * groups, LANES), jnp.float32),
        ],
        scratch_shapes=[
            pltpu.VMEM((length + 8, LANES), jnp.float32),
            pltpu.VMEM((length, LANES), jnp.float32),
            pltpu.VMEM((length, LANES), jnp.float32),
        ],
        name="local_scan",
    )(x, edge, taps, rmap, imap, soft, jump)


def branch_kernel(
    me_ref, arrived, seg, cum_hbm, loc_hbm, gate_hbm, w_ref, *rest, turns
):
    outs, (cum, loc, gates, carry, state, sems) = rest[:-6], rest[-6:]
    rows, channels = state.shape
    groups = channels // LANES
    per_block = SEGMENTS // BLOCKS
    seg_rows = rows // per_block
    starts = [lax.rem(me_ref[0] + steps, BLOCKS) for steps in turns]
    copies = []
    for b, block in enumerate(starts):
        at = pl.ds(pl.multiple_of(block * rows, rows), rows)
        for k, (source, target) in enumerate(((cum_hbm, cum), (loc_hbm, loc), (gate_hbm, gates))):
            copies.append(pltpu.make_async_copy(source.at[at, :], target.at[b], sems.at[3 * b + k]))
    for copy in copies:
        copy.start()

    def join(j, state):
        return arrived[j, 0:groups, :] * state + arrived[j, groups : 2 * groups, :]

    before = lax.fori_loop(0, me_ref[1], join, jnp.zeros((groups, LANES), jnp.float32))
    for g in range(groups):
        lanes = slice(g * LANES, (g + 1) * LANES)
        now = before[g : g + 1, :]
        for s in range(SEGMENTS):
            carry[s, 0:1, lanes] = now
            now = seg[0, s : s + 1, lanes] * now + seg[1, s : s + 1, lanes]
    for copy in copies:
        copy.wait()

    for b, block in enumerate(starts):
        for part in range(per_block):
            at = slice(part * seg_rows, (part + 1) * seg_rows)
            state[at, :] = loc[b, at, :] + cum[b, at, :] * carry[block * per_block + part, 0:1, :]
        out = (state[...] * gelu(gates[b].astype(jnp.float32))).astype(jnp.bfloat16)
        put(outs, b, jnp.dot(out, w_ref[...], preferred_element_type=jnp.float32))


def put(outs, block, share):
    share = share.astype(jnp.bfloat16)
    half = share.shape[1] // 2
    if block < 2:
        outs[2 * block][...] = share[:, :half]
        outs[2 * block + 1][...] = share[:, half:]
    else:
        outs[4][...] = share


VMEM = pl.BlockSpec(memory_space=pltpu.VMEM)
HERE = pl.BlockSpec(memory_space=pltpu.HBM)
OPPOSITE, OTHERS = (2,), (1, 3, 0)


def vm(value):
    return pltpu.with_memory_space_constraint(value, pltpu.VMEM)


def hbm(value):
    return pltpu.with_memory_space_constraint(value, pltpu.HBM)


def vm_out(shape):
    return pltpu.VMEM(shape, jnp.bfloat16)


def share_shapes(turns, rows, width):
    half = vm_out((rows, width // 2))
    return [half] * 2 if len(turns) == 1 else [half] * 4 + [vm_out((rows, width))]


def branch_shares(me, arrived, seg, cum, loc, gate, weight, turns):
    length, channels = cum.shape
    width = weight.shape[1]
    rows = length // BLOCKS
    count = len(turns)
    out_shape = share_shapes(turns, rows, width)
    return pl.pallas_call(
        functools.partial(branch_kernel, turns=turns),
        in_specs=[pl.BlockSpec(memory_space=pltpu.SMEM), VMEM, VMEM, *[HERE] * 3, VMEM],
        out_specs=[VMEM] * len(out_shape),
        out_shape=out_shape,
        scratch_shapes=[
            pltpu.VMEM((count, rows, channels), jnp.float32),
            pltpu.VMEM((count, rows, channels), jnp.float32),
            pltpu.VMEM((count, rows, channels), jnp.bfloat16),
            pltpu.VMEM((SEGMENTS, 1, channels), jnp.float32),
            pltpu.VMEM((rows, channels), jnp.float32),
            pltpu.SemaphoreType.DMA((3 * count,)),
        ],
        cost_estimate=pl.CostEstimate(
            flops=2 * count * rows * channels * width,
            bytes_accessed=count * rows * (10 * channels + 2 * width) + 2 * channels * width,
            transcendentals=count * rows * channels,
        ),
        compiler_params=pltpu.CompilerParams(vmem_limit_bytes=16 * MIB),
        name="branch_first" if count == 1 else "branch_rest",
    )(me, arrived, seg, hbm(cum), hbm(loc), hbm(gate), weight)


def feed_kernel(*refs, turns):
    first = len(turns) == 1
    me_ref, outside = refs[:2]
    halves = {0: refs[2:4], 1: refs[4:6], 2: refs[6:8], 3: refs[8:10]}
    if first:
        weights, gk_ref, vk_ref, *outs, ring, down, lhs, up_a, up_b, act, sems = refs[10:]
    else:
        ring, down, gk_ref, vk_ref, *outs, lhs, up_a, up_b, act = refs[10:]
    rows = halves[0][0].shape[0]
    tall = rows + HALO
    taps = gk_ref.shape[0]
    shards, chunks, shard_rows, _ = down.shape
    width = shards * shard_rows
    half = width // 2
    columns = (slice(0, half), slice(half, width))

    def get(chunk):
        return pltpu.make_async_copy(weights.at[:, pl.ds(2 * chunk, 2)], ring.at[chunk], sems.at[chunk])

    def fill(b, steps):
        at = b * tall
        for part, behind in zip(columns, halves[(steps - 1) % BLOCKS]):
            lhs[at : at + HALO, part] = behind[rows - HALO : rows, :]

        @pl.when(lax.rem(me_ref[0] + steps, BLOCKS) == 0)
        def _():
            lhs[at : at + HALO, :] = outside[...]

        for part, own in zip(columns, halves[steps]):
            lhs[at + HALO : at + tall, part] = own[...]

    def activate(chunk, up):
        lanes = pl.ds(pl.multiple_of(chunk * LANES, LANES), LANES)
        gate_taps = gk_ref[:, lanes].astype(jnp.float32)
        value_taps = vk_ref[:, lanes].astype(jnp.float32)
        for b in range(len(turns)):
            gate = jnp.zeros((rows, LANES), jnp.float32)
            value = jnp.zeros((rows, LANES), jnp.float32)
            for k in range(taps):
                at = b * tall + HALO - (taps - 1) + k
                gate = gate + up[at : at + rows, 0:LANES] * gate_taps[k : k + 1, :]
                value = value + up[at : at + rows, LANES : 2 * LANES] * value_taps[k : k + 1, :]
            act[b * rows : (b + 1) * rows, lanes] = (gelu(gate) * value).astype(jnp.bfloat16)

    def project(chunk, up):
        sides = [ring[chunk, :, side].reshape(width, LANES) for side in range(2)]
        up[...] = (
            jnp.dot(lhs[...], jnp.concatenate(sides, axis=1), preferred_element_type=jnp.float32)
            .astype(jnp.bfloat16)
            .astype(jnp.float32)
        )

    if first:
        get_down = pltpu.make_async_copy(weights.at[:, pl.ds(2 * chunks, chunks)], down, sems.at[chunks])
        for chunk in range(chunks):
            get(jnp.int32(chunk)).start()
        get_down.start()
    for b, steps in enumerate(turns):
        fill(b, steps)
    if first:
        get(jnp.int32(0)).wait()
    project(jnp.int32(0), up_a)

    def pair(i, carry):
        chunk = 2 * i
        if first:
            get(chunk + 1).wait()
            get(chunk + 2).wait()
        activate(chunk, up_a)
        project(chunk + 1, up_b)
        activate(chunk + 1, up_b)
        project(chunk + 2, up_a)
        return carry

    lax.fori_loop(0, chunks // 2, pair, 0)
    if first:
        get_down.wait()
    activate(jnp.int32(chunks - 1), up_a)
    turned = jnp.concatenate([down[:, c].reshape(width, LANES) for c in range(chunks)], axis=1)
    share = lax.dot_general(
        act[...], turned, (((1,), (1,)), ((), ())), preferred_element_type=jnp.float32
    )
    for b in range(len(turns)):
        put(outs, b, share[b * rows : (b + 1) * rows, :])


def feed(me, outside, halves, weights, gate_kernel, value_kernel, turns):
    first = len(turns) == 1
    count = len(turns)
    rows, half = halves[0].shape
    width, units = 2 * half, gate_kernel.shape[1]
    chunks = units // LANES
    assert chunks % 2 == 1
    tall = count * (rows + HALO)
    out_shape = share_shapes(turns, rows, width)
    scratch = [
        pltpu.VMEM((tall, width), jnp.bfloat16),
        pltpu.VMEM((tall, 2 * LANES), jnp.float32),
        pltpu.VMEM((tall, 2 * LANES), jnp.float32),
        pltpu.VMEM((count * rows, units), jnp.bfloat16),
    ]
    if first:
        shards, _, shard_rows, _ = weights[0].shape
        out_shape += [
            vm_out((chunks, shards, 2, shard_rows, LANES)),
            vm_out((shards, chunks, shard_rows, LANES)),
        ]
        scratch += [pltpu.SemaphoreType.DMA((chunks + 1,))]
    else:
        weights = map(vm, weights)
    return pl.pallas_call(
        functools.partial(feed_kernel, turns=turns),
        in_specs=[
            pl.BlockSpec(memory_space=pltpu.SMEM),
            *[VMEM] * (1 + len(halves)),
            *([HERE] if first else [VMEM] * 2),
            VMEM,
            VMEM,
        ],
        out_specs=[VMEM] * len(out_shape),
        out_shape=out_shape,
        scratch_shapes=scratch,
        cost_estimate=pl.CostEstimate(
            flops=6 * count * rows * width * units,
            bytes_accessed=6 * width * units + 4 * count * rows * width,
            transcendentals=count * rows * units,
        ),
        compiler_params=pltpu.CompilerParams(vmem_limit_bytes=12 * MIB),
        name="feed_first" if first else "feed_rest",
    )(me, vm(outside), *map(vm, halves), *weights, gate_kernel, value_kernel)


def pack_kernel(gate_ref, value_ref, turned_ref, out_ref):
    chunks = gate_ref.shape[1] // LANES
    for c in range(chunks):
        lanes = slice(c * LANES, (c + 1) * LANES)
        out_ref[2 * c] = gate_ref[:, lanes]
        out_ref[2 * c + 1] = value_ref[:, lanes]
        out_ref[2 * chunks + c] = turned_ref[:, lanes]


def packed(gate, value, turned):
    rows, units = gate.shape
    return pl.pallas_call(
        pack_kernel,
        out_shape=jax.ShapeDtypeStruct((3 * units // LANES, rows, LANES), jnp.bfloat16),
        name="pack",
    )(gate, value, turned)


def scaled(v, gain):
    return v * lax.rsqrt(jnp.mean(v * v, axis=-1, keepdims=True) + EPS) * gain


def shares_sum(refs, at):
    own, left_low, left_high, right_low, right_high = refs
    half = left_low.shape[1]
    parts = []
    for part, left, right in (
        (slice(0, half), left_low, right_low),
        (slice(half, 2 * half), left_high, right_high),
    ):
        total = own[at, part].astype(jnp.float32) + left[at, :].astype(jnp.float32)
        total = total + right[at, :].astype(jnp.float32)
        parts.append(total.astype(jnp.bfloat16).astype(jnp.float32))
    return jnp.concatenate(parts, axis=1)


def by_rows(rows, body):
    def step(i, carry):
        body(pl.ds(pl.multiple_of(i * HALO, HALO), HALO))
        return carry

    lax.fori_loop(0, rows // HALO, step, 0)


def mid_kernel(me_ref, *refs):
    shares, (res_hbm, mix_ref, inner_ref, hidden_ref, low_ref, high_ref, res, sem) = refs[:5], refs[5:]
    rows, half = low_ref.shape
    first = pl.multiple_of(me_ref[0] * rows, rows)
    fetch = pltpu.make_async_copy(res_hbm.at[pl.ds(first, rows), :], res, sem)
    fetch.start()
    mix, inner = mix_ref[...], inner_ref[...]
    fetch.wait()

    def body(at):
        hidden = (
            res[at, :].astype(jnp.float32) + scaled(shares_sum(shares, at), mix)
        ).astype(jnp.bfloat16)
        hidden_ref[at, :] = hidden
        normed = scaled(hidden.astype(jnp.float32), inner).astype(jnp.bfloat16)
        low_ref[at, :] = normed[:, :half]
        high_ref[at, :] = normed[:, half:]

    by_rows(rows, body)


def mid(me, shares, residual, mix_gain, inner_gain):
    rows, width = shares[0].shape
    return pl.pallas_call(
        mid_kernel,
        in_specs=[pl.BlockSpec(memory_space=pltpu.SMEM), *[VMEM] * 5, HERE, VMEM, VMEM],
        out_specs=[VMEM] * 3,
        out_shape=[
            jax.ShapeDtypeStruct((rows, width), jnp.bfloat16),
            *[vm_out((rows, width // 2))] * 2,
        ],
        scratch_shapes=[pltpu.VMEM((rows, width), jnp.bfloat16), pltpu.SemaphoreType.DMA],
        compiler_params=pltpu.CompilerParams(vmem_limit_bytes=12 * MIB),
        name="mid",
    )(me, *map(vm, shares), hbm(residual), mix_gain, inner_gain)


def last_kernel(*refs):
    shares, (hidden_ref, gain_ref, out_ref) = refs[:5], refs[5:]
    gain = gain_ref[...]

    def body(at):
        out_ref[at, :] = (
            hidden_ref[at, :].astype(jnp.float32) + scaled(shares_sum(shares, at), gain)
        ).astype(jnp.bfloat16)

    by_rows(hidden_ref.shape[0], body)


def last(shares, hidden, gain):
    return pl.pallas_call(
        last_kernel,
        in_specs=[VMEM] * 7,
        out_specs=VMEM,
        out_shape=jax.ShapeDtypeStruct(hidden.shape, jnp.bfloat16),
        compiler_params=pltpu.CompilerParams(vmem_limit_bytes=12 * MIB),
        name="last",
    )(*map(vm, shares), hidden, gain)


def join_kernel(right_low, low_ref, left_high, high_ref, right_ref, left_ref):
    def body(at):
        for own, other, out in ((right_low, low_ref, right_ref), (left_high, high_ref, left_ref)):
            total = own[at, :].astype(jnp.float32) + other[at, :].astype(jnp.float32)
            out[at, :] = total.astype(jnp.bfloat16)

    by_rows(low_ref.shape[0], body)


def join(right_low, low, left_high, high):
    return pl.pallas_call(
        join_kernel,
        in_specs=[VMEM] * 4,
        out_specs=[VMEM] * 2,
        out_shape=[vm_out(low.shape)] * 2,
        compiler_params=pltpu.CompilerParams(vmem_limit_bytes=12 * MIB),
        name="join",
    )(*map(vm, (right_low, low, left_high, high)))


def turn(value, axis, steps):
    count = lax.axis_size(axis)
    return lax.ppermute(value, axis, [(i, (i + steps) % count) for i in range(count)])


def ring_sum(first, rest):
    low, high = turn(first[0], "tp", 1), turn(first[1], "tp", -1)
    right_low, right_high, left_low, left_high, own = rest
    from_left_high, from_right_low = turn(right_high, "tp", 1), turn(left_low, "tp", -1)
    right_low, left_high = join(right_low, low, left_high, high)
    from_left_low, from_right_high = turn(right_low, "tp", 1), turn(left_high, "tp", -1)
    return own, from_left_low, from_left_high, from_right_low, from_right_high


def from_behind(value, axis):
    count = lax.axis_size(axis)
    return lax.ppermute(value, axis, [(i, i + 1) for i in range(count - 1)])


def exchanged(tiles, axis):
    return lax.all_to_all(tiles, axis, split_axis=0, concat_axis=0, tiled=True)


def local(
    residual,
    mix_input,
    gate_input,
    mix_kernel,
    recur_gate_map,
    input_gate_map,
    decay_param,
    jump_log,
    out_weight,
    mix_gain,
    inner_gain,
    final_gain,
    gate_weight,
    value_weight,
    gate_kernel,
    value_kernel,
    down_weight,
):
    n_tp, n_sp = lax.axis_size("tp"), lax.axis_size("sp")
    assert n_tp == BLOCKS
    tp_me = lax.axis_index("tp").astype(jnp.int32)
    me = jnp.stack([tp_me, lax.axis_index("sp").astype(jnp.int32)])

    edge = from_behind(mix_input[mix_input.shape[0] - 8 :], "sp")
    shard = packed(gate_weight, value_weight, down_weight.T)
    weights = lax.all_gather(shard, "sp", axis=0, tiled=True).reshape(n_sp, *shard.shape)

    cum, loc, seg, ends = local_scan(
        mix_input, edge, mix_kernel, recur_gate_map, input_gate_map, decay_param[None], jump_log, n_sp
    )
    arrived = exchanged(ends, "sp")
    shares = functools.partial(
        branch_shares, arrived=arrived, seg=seg, cum=cum, loc=loc, gate=gate_input, weight=out_weight
    )
    first = shares(me, turns=OPPOSITE)
    rest = shares(me, turns=OTHERS)
    hidden_state, own_low, own_high = mid(
        me, ring_sum(first, rest), residual, mix_gain[None], inner_gain[None]
    )
    left_low, right_high = turn(own_low, "tp", 1), turn(own_high, "tp", -1)
    left_high, right_low = turn(own_high, "tp", 1), turn(own_low, "tp", -1)
    opposite_low, opposite_high = turn(left_low, "tp", 1), turn(right_high, "tp", -1)

    tail = lambda low, high: jnp.concatenate([low[-HALO:], high[-HALO:]], axis=1)
    own_tail = tail(own_low, own_high)
    final_tail = jnp.where(
        tp_me == n_tp - 1,
        own_tail,
        jnp.where(tp_me == 0, tail(left_low, left_high), tail(right_low, right_high)),
    )
    places = range(n_sp - 1)
    outside = jnp.where(
        tp_me == 1,
        lax.ppermute(own_tail, ("sp", "tp"), [(s * n_tp + n_tp - 1, (s + 1) * n_tp + 1) for s in places]),
        lax.ppermute(
            final_tail,
            ("sp", "tp"),
            [(s * n_tp + t, (s + 1) * n_tp + t) for s in places for t in (0, 2, 3)],
        ),
    )
    halves = (own_low, own_high, right_low, right_high, opposite_low, opposite_high, left_low, left_high)
    *first, ring, down = feed(
        me, outside, halves, (hbm(weights),), gate_kernel, value_kernel, turns=OPPOSITE
    )
    rest = feed(me, outside, halves, (ring, down), gate_kernel, value_kernel, turns=OTHERS)
    return last(ring_sum(first, rest), hidden_state, final_gain[None])


def solution(mesh):
    return jax.shard_map(
        local,
        mesh=mesh,
        in_specs=(
            P(("grp", "sp"), None),
            P(("grp", "sp"), "tp"),
            P(("grp", "sp"), "tp"),
            P(None, "tp"),
            P("tp", None, None),
            P("tp", None, None),
            P("tp"),
            P(("grp", "sp"), "tp"),
            P("tp", None),
            P(),
            P(),
            P(),
            P("sp", "tp"),
            P("sp", "tp"),
            P(None, "tp"),
            P(None, "tp"),
            P("tp", "sp"),
        ),
        out_specs=P(("grp", "sp", "tp"), None),
        check_vma=False,
    )
```

```python
import functools

import jax
import jax.numpy as jnp
from jax import lax
from jax.experimental import pallas as pl
from jax.experimental.pallas import tpu as pltpu
from jax.sharding import PartitionSpec as P

EPS = 1e-06
GATE_SCALE = 8.0
SEGMENTS = 8
LANES = 128
BLOCKS = 4
HALO = 16
MIB = 1 << 20
GELU_A = 0.7978845608028654
GELU_B = 0.044715


def gelu(v):
    return 0.5 * v * (1.0 + jnp.tanh(GELU_A * (v + GELU_B * (v * v * v))))


def minus_expm1(y):
    series = 1.0 + y * (1.0 / 7.0)
    for n in (6.0, 5.0, 4.0, 3.0, 2.0):
        series = 1.0 + y * (1.0 / n) * series
    return jnp.where(y > -0.3, -y * series, 1.0 - jnp.exp(y))


def sigmoid(v):
    return 0.5 * jnp.tanh(0.5 * v) + 0.5


def scan_kernel(
    x_ref, edge_ref, taps_ref, rmap_ref, imap_ref, soft_ref, jump_ref,
    cum_ref, loc_ref, seg_ref, ends_ref,
    xs, decay, drive,
):
    group = pl.program_id(0)
    groups = pl.num_programs(0)
    length = x_ref.shape[0]
    taps = taps_ref.shape[0]
    xs[0:8, :] = edge_ref[...].astype(jnp.float32)
    xs[8 : 8 + length, :] = x_ref[...].astype(jnp.float32)
    rows = length // 4
    kernel = taps_ref[...].astype(jnp.float32)
    v = -soft_ref[...]
    soft = jnp.maximum(v, 0.0) + jnp.log1p(jnp.exp(-jnp.abs(v)))
    for at in range(0, length, rows):
        conv = jnp.zeros((rows, LANES), jnp.float32)
        for k in range(taps):
            first = 8 + at - (taps - 1) + k
            conv = conv + xs[first : first + rows, :] * kernel[k : k + 1, :]
        conv = conv.astype(jnp.bfloat16)
        rgate = sigmoid(jnp.dot(conv, rmap_ref[0], preferred_element_type=jnp.float32))
        igate = sigmoid(jnp.dot(conv, imap_ref[0], preferred_element_type=jnp.float32))
        log_decay = -GATE_SCALE * rgate * soft + jump_ref[at : at + rows, :]
        decay[at : at + rows, :] = jnp.exp(log_decay)
        drive[at : at + rows, :] = (
            jnp.sqrt(minus_expm1(2.0 * log_decay)) * igate * conv.astype(jnp.float32)
        )
    steps = length // SEGMENTS

    def step(i, carry):
        state, product = carry
        where = pl.ds(i, SEGMENTS, steps)
        a = decay[where, :]
        state = a * state + drive[where, :]
        product = a * product
        loc_ref[where, :] = state
        cum_ref[where, :] = product
        return state, product

    zero = jnp.zeros((SEGMENTS, LANES), jnp.float32)
    state, product = lax.fori_loop(0, steps, step, (zero, zero + 1.0), unroll=8)
    seg_ref[0, :, :] = product
    seg_ref[1, :, :] = state
    all_state = state[0:1]
    all_product = product[0:1]
    for s in range(1, SEGMENTS):
        all_state = product[s : s + 1] * all_state + state[s : s + 1]
        all_product = product[s : s + 1] * all_product
    count = ends_ref.shape[0]
    ends_ref[:, pl.ds(group, 1), :] = jnp.broadcast_to(all_product[None], (count, 1, LANES))
    ends_ref[:, pl.ds(groups + group, 1), :] = jnp.broadcast_to(all_state[None], (count, 1, LANES))


def local_scan(x, edge, taps, rmap, imap, soft, jump, copies):
    length, channels = x.shape
    groups = channels // LANES
    column = lambda rows: pl.BlockSpec((rows, LANES), lambda g: (0, g))
    square = pl.BlockSpec((1, LANES, LANES), lambda g: (g, 0, 0))
    return pl.pallas_call(
        scan_kernel,
        grid=(groups,),
        in_specs=[column(length), column(8), column(taps.shape[0]), square, square, column(1), column(length)],
        out_specs=[
            column(length),
            column(length),
            pl.BlockSpec((2, SEGMENTS, LANES), lambda g: (0, 0, g)),
            pl.BlockSpec((copies, 2 * groups, LANES), lambda g: (0, 0, 0)),
        ],
        out_shape=[
            jax.ShapeDtypeStruct((length, channels), jnp.float32),
            jax.ShapeDtypeStruct((length, channels), jnp.float32),
            jax.ShapeDtypeStruct((2, SEGMENTS, channels), jnp.float32),
            jax.ShapeDtypeStruct((copies, 2 * groups, LANES), jnp.float32),
        ],
        scratch_shapes=[
            pltpu.VMEM((length + 8, LANES), jnp.float32),
            pltpu.VMEM((length, LANES), jnp.float32),
            pltpu.VMEM((length, LANES), jnp.float32),
        ],
        name="local_scan",
    )(x, edge, taps, rmap, imap, soft, jump)


def branch_kernel(
    me_ref, arrived, seg, cum_hbm, loc_hbm, gate_hbm, w_ref, *rest, turns
):
    outs, (cum, loc, gates, carry, state, sems) = rest[:-6], rest[-6:]
    rows, channels = state.shape
    groups = channels // LANES
    per_block = SEGMENTS // BLOCKS
    seg_rows = rows // per_block
    starts = [lax.rem(me_ref[0] + steps, BLOCKS) for steps in turns]
    copies = []
    for b, block in enumerate(starts):
        at = pl.ds(pl.multiple_of(block * rows, rows), rows)
        for k, (source, target) in enumerate(((cum_hbm, cum), (loc_hbm, loc), (gate_hbm, gates))):
            copies.append(pltpu.make_async_copy(source.at[at, :], target.at[b], sems.at[3 * b + k]))
    for copy in copies:
        copy.start()

    def join(j, state):
        return arrived[j, 0:groups, :] * state + arrived[j, groups : 2 * groups, :]

    before = lax.fori_loop(0, me_ref[1], join, jnp.zeros((groups, LANES), jnp.float32))
    for g in range(groups):
        lanes = slice(g * LANES, (g + 1) * LANES)
        now = before[g : g + 1, :]
        for s in range(SEGMENTS):
            carry[s, 0:1, lanes] = now
            now = seg[0, s : s + 1, lanes] * now + seg[1, s : s + 1, lanes]
    for copy in copies:
        copy.wait()

    for b, block in enumerate(starts):
        for part in range(per_block):
            at = slice(part * seg_rows, (part + 1) * seg_rows)
            state[at, :] = loc[b, at, :] + cum[b, at, :] * carry[block * per_block + part, 0:1, :]
        out = (state[...] * gelu(gates[b].astype(jnp.float32))).astype(jnp.bfloat16)
        put(outs, b, turns[b], jnp.dot(out, w_ref[...], preferred_element_type=jnp.float32))


def put(outs, at, steps, share):
    share = share.astype(jnp.bfloat16)
    half = share.shape[1] // 2
    if steps:
        outs[2 * at][...] = share[:, :half]
        outs[2 * at + 1][...] = share[:, half:]
    else:
        outs[2 * at][...] = share


VMEM = pl.BlockSpec(memory_space=pltpu.VMEM)
HERE = pl.BlockSpec(memory_space=pltpu.HBM)
OPPOSITE, SIDES, OTHERS, OWN = (2,), (1, 3), (1, 3, 0), (0,)


def vm(value):
    return pltpu.with_memory_space_constraint(value, pltpu.VMEM)


def hbm(value):
    return pltpu.with_memory_space_constraint(value, pltpu.HBM)


def hbm_out(shape):
    return pltpu.HBM(shape, jnp.bfloat16)


def vm_out(shape):
    return pltpu.VMEM(shape, jnp.bfloat16)


def share_shapes(turns, rows, width):
    half = vm_out((rows, width // 2))
    return sum(([half] * 2 if steps else [vm_out((rows, width))] for steps in turns), [])


def branch_shares(me, arrived, seg, cum, loc, gate, weight, turns):
    length, channels = cum.shape
    width = weight.shape[1]
    rows = length // BLOCKS
    count = len(turns)
    out_shape = share_shapes(turns, rows, width)
    return pl.pallas_call(
        functools.partial(branch_kernel, turns=turns),
        in_specs=[pl.BlockSpec(memory_space=pltpu.SMEM), VMEM, VMEM, *[HERE] * 3, VMEM],
        out_specs=[VMEM] * len(out_shape),
        out_shape=out_shape,
        scratch_shapes=[
            pltpu.VMEM((count, rows, channels), jnp.float32),
            pltpu.VMEM((count, rows, channels), jnp.float32),
            pltpu.VMEM((count, rows, channels), jnp.bfloat16),
            pltpu.VMEM((SEGMENTS, 1, channels), jnp.float32),
            pltpu.VMEM((rows, channels), jnp.float32),
            pltpu.SemaphoreType.DMA((3 * count,)),
        ],
        cost_estimate=pl.CostEstimate(
            flops=2 * count * rows * channels * width,
            bytes_accessed=count * rows * (10 * channels + 2 * width) + 2 * channels * width,
            transcendentals=count * rows * channels,
        ),
        compiler_params=pltpu.CompilerParams(vmem_limit_bytes=16 * MIB),
        name="branch_first" if count == 1 else "branch_rest",
    )(me, arrived, seg, hbm(cum), hbm(loc), hbm(gate), weight)


def feed_kernel(*refs, turns):
    first = turns == OPPOSITE
    me_ref, outside = refs[:2]
    halves = {0: refs[2:4], 1: refs[4:6], 2: refs[6:8], 3: refs[8:10]}
    if first:
        weights, gk_ref, vk_ref, *outs, ring, down, lhs, up, act, sems = refs[10:]
    else:
        ring, down, gk_ref, vk_ref, *outs, lhs, up, act = refs[10:]
    rows = halves[0][0].shape[0]
    tall = rows + HALO
    taps = gk_ref.shape[0]
    shards, chunks, shard_rows, _ = down.shape
    width = shards * shard_rows
    half = width // 2
    columns = (slice(0, half), slice(half, width))

    def get(chunk):
        return pltpu.make_async_copy(weights.at[:, pl.ds(2 * chunk, 2)], ring.at[chunk], sems.at[chunk])

    def fill(b, steps):
        at = b * tall
        for part, behind in zip(columns, halves[(steps - 1) % BLOCKS]):
            lhs[at : at + HALO, part] = behind[rows - HALO : rows, :]

        @pl.when(lax.rem(me_ref[0] + steps, BLOCKS) == 0)
        def _():
            lhs[at : at + HALO, :] = outside[...]

        for part, own in zip(columns, halves[steps]):
            lhs[at + HALO : at + tall, part] = own[...]

    def activate(chunk):
        side = lax.rem(chunk, 2)
        lanes = pl.ds(pl.multiple_of(chunk * LANES, LANES), LANES)
        gate_taps = gk_ref[:, lanes].astype(jnp.float32)
        value_taps = vk_ref[:, lanes].astype(jnp.float32)
        for b in range(len(turns)):
            gate = jnp.zeros((rows, LANES), jnp.float32)
            value = jnp.zeros((rows, LANES), jnp.float32)
            for k in range(taps):
                at = b * tall + HALO - (taps - 1) + k
                gate = gate + up[side, at : at + rows, 0:LANES] * gate_taps[k : k + 1, :]
                value = value + up[side, at : at + rows, LANES : 2 * LANES] * value_taps[k : k + 1, :]
            act[b * rows : (b + 1) * rows, lanes] = (gelu(gate) * value).astype(jnp.bfloat16)

    def project(chunk):
        sides = [ring[chunk, :, side].reshape(width, LANES) for side in range(2)]
        up[lax.rem(chunk, 2)] = (
            jnp.dot(lhs[...], jnp.concatenate(sides, axis=1), preferred_element_type=jnp.float32)
            .astype(jnp.bfloat16)
            .astype(jnp.float32)
        )

    if first:
        get_down = pltpu.make_async_copy(weights.at[:, pl.ds(2 * chunks, chunks)], down, sems.at[chunks])
        for chunk in range(chunks):
            get(jnp.int32(chunk)).start()
        get_down.start()
    for b, steps in enumerate(turns):
        fill(b, steps)
    if first:
        get(jnp.int32(0)).wait()
    project(jnp.int32(0))

    def step(chunk, carry):
        if first:
            get(chunk + 1).wait()
        activate(chunk)
        project(chunk + 1)
        return carry

    lax.fori_loop(0, chunks - 1, step, 0)
    if first:
        get_down.wait()
    activate(jnp.int32(chunks - 1))
    turned = jnp.concatenate([down[:, c].reshape(width, LANES) for c in range(chunks)], axis=1)
    share = lax.dot_general(
        act[...], turned, (((1,), (1,)), ((), ())), preferred_element_type=jnp.float32
    )
    for b in range(len(turns)):
        put(outs, b, turns[b], share[b * rows : (b + 1) * rows, :])


def feed(me, outside, halves, weights, gate_kernel, value_kernel, turns):
    first = turns == OPPOSITE
    count = len(turns)
    rows, half = halves[0].shape
    width, units = 2 * half, gate_kernel.shape[1]
    chunks = units // LANES
    tall = count * (rows + HALO)
    out_shape = share_shapes(turns, rows, width)
    scratch = [
        pltpu.VMEM((tall, width), jnp.bfloat16),
        pltpu.VMEM((2, tall, 2 * LANES), jnp.float32),
        pltpu.VMEM((count * rows, units), jnp.bfloat16),
    ]
    if first:
        shards, _, shard_rows, _ = weights[0].shape
        out_shape += [
            vm_out((chunks, shards, 2, shard_rows, LANES)),
            vm_out((shards, chunks, shard_rows, LANES)),
        ]
        scratch += [pltpu.SemaphoreType.DMA((chunks + 1,))]
    else:
        weights = map(vm, weights)
    return pl.pallas_call(
        functools.partial(feed_kernel, turns=turns),
        in_specs=[
            pl.BlockSpec(memory_space=pltpu.SMEM),
            *[VMEM] * (1 + len(halves)),
            *([HERE] if first else [VMEM] * 2),
            VMEM,
            VMEM,
        ],
        out_specs=[VMEM] * len(out_shape),
        out_shape=out_shape,
        scratch_shapes=scratch,
        cost_estimate=pl.CostEstimate(
            flops=6 * count * rows * width * units,
            bytes_accessed=6 * width * units + 4 * count * rows * width,
            transcendentals=count * rows * units,
        ),
        compiler_params=pltpu.CompilerParams(vmem_limit_bytes=12 * MIB),
        name={OPPOSITE: "feed_first", SIDES: "feed_sides", OWN: "feed_own"}[turns],
    )(me, outside, *map(vm, halves[:4]), *halves[4:6], *map(vm, halves[6:]), *weights, gate_kernel, value_kernel)


def pack_kernel(gate_ref, value_ref, turned_ref, out_ref):
    chunks = gate_ref.shape[1] // LANES
    for c in range(chunks):
        lanes = slice(c * LANES, (c + 1) * LANES)
        out_ref[2 * c] = gate_ref[:, lanes]
        out_ref[2 * c + 1] = value_ref[:, lanes]
        out_ref[2 * chunks + c] = turned_ref[:, lanes]


def packed(gate, value, turned):
    rows, units = gate.shape
    return pl.pallas_call(
        pack_kernel,
        out_shape=jax.ShapeDtypeStruct((3 * units // LANES, rows, LANES), jnp.bfloat16),
        name="pack",
    )(gate, value, turned)


def scaled(v, gain):
    return v * lax.rsqrt(jnp.mean(v * v, axis=-1, keepdims=True) + EPS) * gain


def shares_sum(refs, at):
    own, left_low, left_high, right_low, right_high = refs
    half = left_low.shape[1]
    parts = []
    for part, left, right in (
        (slice(0, half), left_low, right_low),
        (slice(half, 2 * half), left_high, right_high),
    ):
        total = own[at, part].astype(jnp.float32) + left[at, :].astype(jnp.float32)
        total = total + right[at, :].astype(jnp.float32)
        parts.append(total.astype(jnp.bfloat16).astype(jnp.float32))
    return jnp.concatenate(parts, axis=1)


def by_rows(rows, body):
    def step(i, carry):
        body(pl.ds(pl.multiple_of(i * HALO, HALO), HALO))
        return carry

    lax.fori_loop(0, rows // HALO, step, 0)


def mid_kernel(me_ref, *refs):
    shares, (res_hbm, mix_ref, inner_ref, hidden_ref, low_ref, high_ref, res, sem) = refs[:5], refs[5:]
    rows, half = low_ref.shape
    first = pl.multiple_of(me_ref[0] * rows, rows)
    fetch = pltpu.make_async_copy(res_hbm.at[pl.ds(first, rows), :], res, sem)
    fetch.start()
    mix, inner = mix_ref[...], inner_ref[...]
    fetch.wait()

    def body(at):
        hidden = (
            res[at, :].astype(jnp.float32) + scaled(shares_sum(shares, at), mix)
        ).astype(jnp.bfloat16)
        hidden_ref[at, :] = hidden
        normed = scaled(hidden.astype(jnp.float32), inner).astype(jnp.bfloat16)
        low_ref[at, :] = normed[:, :half]
        high_ref[at, :] = normed[:, half:]

    by_rows(rows, body)


def mid(me, shares, residual, mix_gain, inner_gain):
    rows, width = shares[0].shape
    return pl.pallas_call(
        mid_kernel,
        in_specs=[pl.BlockSpec(memory_space=pltpu.SMEM), *[VMEM] * 5, HERE, VMEM, VMEM],
        out_specs=[VMEM] * 3,
        out_shape=[
            hbm_out((rows, width)),
            *[vm_out((rows, width // 2))] * 2,
        ],
        scratch_shapes=[pltpu.VMEM((rows, width), jnp.bfloat16), pltpu.SemaphoreType.DMA],
        compiler_params=pltpu.CompilerParams(vmem_limit_bytes=12 * MIB),
        name="mid",
    )(me, *map(vm, shares), hbm(residual), mix_gain, inner_gain)


def last_kernel(*refs):
    shares, (hidden_ref, gain_ref, out_ref) = refs[:5], refs[5:]
    gain = gain_ref[...]

    def body(at):
        out_ref[at, :] = (
            hidden_ref[at, :].astype(jnp.float32) + scaled(shares_sum(shares, at), gain)
        ).astype(jnp.bfloat16)

    by_rows(hidden_ref.shape[0], body)


def last(shares, hidden, gain):
    return pl.pallas_call(
        last_kernel,
        in_specs=[VMEM] * 7,
        out_specs=VMEM,
        out_shape=jax.ShapeDtypeStruct(hidden.shape, jnp.bfloat16),
        compiler_params=pltpu.CompilerParams(vmem_limit_bytes=12 * MIB),
        name="last",
    )(*map(vm, shares), hidden, gain)


def join_kernel(right_low, low_ref, left_high, high_ref, right_ref, left_ref):
    def body(at):
        for own, other, out in ((right_low, low_ref, right_ref), (left_high, high_ref, left_ref)):
            total = own[at, :].astype(jnp.float32) + other[at, :].astype(jnp.float32)
            out[at, :] = total.astype(jnp.bfloat16)

    by_rows(low_ref.shape[0], body)


def join(right_low, low, left_high, high):
    return pl.pallas_call(
        join_kernel,
        in_specs=[VMEM] * 4,
        out_specs=[VMEM] * 2,
        out_shape=[vm_out(low.shape)] * 2,
        compiler_params=pltpu.CompilerParams(vmem_limit_bytes=12 * MIB),
        name="join",
    )(*map(vm, (right_low, low, left_high, high)))


def turn(value, axis, steps):
    count = lax.axis_size(axis)
    return lax.ppermute(value, axis, [(i, (i + steps) % count) for i in range(count)])


def ring_sum(first, rest):
    low, high = turn(first[0], "tp", 1), turn(first[1], "tp", -1)
    right_low, right_high, left_low, left_high, own = rest
    from_left_high, from_right_low = turn(right_high, "tp", 1), turn(left_low, "tp", -1)
    right_low, left_high = join(right_low, low, left_high, high)
    from_left_low, from_right_high = turn(right_low, "tp", 1), turn(left_high, "tp", -1)
    return own, from_left_low, from_left_high, from_right_low, from_right_high


def from_behind(value, axis):
    count = lax.axis_size(axis)
    return lax.ppermute(value, axis, [(i, i + 1) for i in range(count - 1)])


def exchanged(tiles, axis):
    return lax.all_to_all(tiles, axis, split_axis=0, concat_axis=0, tiled=True)


def local(
    residual,
    mix_input,
    gate_input,
    mix_kernel,
    recur_gate_map,
    input_gate_map,
    decay_param,
    jump_log,
    out_weight,
    mix_gain,
    inner_gain,
    final_gain,
    gate_weight,
    value_weight,
    gate_kernel,
    value_kernel,
    down_weight,
):
    n_tp, n_sp = lax.axis_size("tp"), lax.axis_size("sp")
    assert n_tp == BLOCKS
    tp_me = lax.axis_index("tp").astype(jnp.int32)
    me = jnp.stack([tp_me, lax.axis_index("sp").astype(jnp.int32)])

    edge = from_behind(mix_input[mix_input.shape[0] - 8 :], "sp")
    shard = packed(gate_weight, value_weight, down_weight.T)
    weights = lax.all_gather(shard, "sp", axis=0, tiled=True).reshape(n_sp, *shard.shape)

    cum, loc, seg, ends = local_scan(
        mix_input, edge, mix_kernel, recur_gate_map, input_gate_map, decay_param[None], jump_log, n_sp
    )
    arrived = exchanged(ends, "sp")
    shares = functools.partial(
        branch_shares, arrived=arrived, seg=seg, cum=cum, loc=loc, gate=gate_input, weight=out_weight
    )
    first = shares(me, turns=OPPOSITE)
    rest = shares(me, turns=OTHERS)
    hidden_state, own_low, own_high = mid(
        me, ring_sum(first, rest), residual, mix_gain[None], inner_gain[None]
    )
    left_low, right_high = turn(own_low, "tp", 1), turn(own_high, "tp", -1)
    left_high, right_low = turn(own_high, "tp", 1), turn(own_low, "tp", -1)
    opposite_low, opposite_high = turn(left_low, "tp", 1), turn(right_high, "tp", -1)

    tail = lambda low, high: jnp.concatenate([low[-HALO:], high[-HALO:]], axis=1)
    own_tail = tail(own_low, own_high)
    final_tail = jnp.where(
        tp_me == n_tp - 1,
        own_tail,
        jnp.where(tp_me == 0, tail(left_low, left_high), tail(right_low, right_high)),
    )
    places = range(n_sp - 1)
    outside = jnp.where(
        tp_me == 1,
        lax.ppermute(own_tail, ("sp", "tp"), [(s * n_tp + n_tp - 1, (s + 1) * n_tp + 1) for s in places]),
        lax.ppermute(
            final_tail,
            ("sp", "tp"),
            [(s * n_tp + t, (s + 1) * n_tp + t) for s in places for t in (0, 2, 3)],
        ),
    )
    halves = (own_low, own_high, right_low, right_high, opposite_low, opposite_high, left_low, left_high)
    *first, ring, down = feed(
        me, outside, halves, (hbm(weights),), gate_kernel, value_kernel, turns=OPPOSITE
    )
    given = (me, outside, halves, (ring, down), gate_kernel, value_kernel)
    rest = feed(*given, turns=SIDES) + feed(*given, turns=OWN)
    return last(ring_sum(first, rest), hidden_state, final_gain[None])


def solution(mesh):
    return jax.shard_map(
        local,
        mesh=mesh,
        in_specs=(
            P(("grp", "sp"), None),
            P(("grp", "sp"), "tp"),
            P(("grp", "sp"), "tp"),
            P(None, "tp"),
            P("tp", None, None),
            P("tp", None, None),
            P("tp"),
            P(("grp", "sp"), "tp"),
            P("tp", None),
            P(),
            P(),
            P(),
            P("sp", "tp"),
            P("sp", "tp"),
            P(None, "tp"),
            P(None, "tp"),
            P("tp", "sp"),
        ),
        out_specs=P(("grp", "sp", "tp"), None),
        check_vma=False,
    )
```

```python
import functools

import jax
import jax.numpy as jnp
from jax import lax
from jax.experimental import pallas as pl
from jax.experimental.pallas import tpu as pltpu
from jax.sharding import PartitionSpec as P


EPS = 1e-06
GATE_SCALE = 8.0
SEGMENTS = 8
LANES = 128
BLOCKS = 4
HALO = 16
MIB = 1 << 20
GELU_A = 0.7978845608028654
GELU_B = 0.044715


def gelu(v):
    return 0.5 * v * (1.0 + jnp.tanh(GELU_A * (v + GELU_B * (v * v * v))))


def minus_expm1(y):
    series = 1.0 + y * (1.0 / 7.0)
    for n in (6.0, 5.0, 4.0, 3.0, 2.0):
        series = 1.0 + y * (1.0 / n) * series
    return jnp.where(y > -0.3, -y * series, 1.0 - jnp.exp(y))


def sigmoid(v):
    return 0.5 * jnp.tanh(0.5 * v) + 0.5


def scan_kernel(
    x_ref, edge_ref, taps_ref, rmap_ref, imap_ref, soft_ref, jump_ref,
    cum_ref, loc_ref, seg_ref, ends_ref,
    xs, decay, drive,
):
    group = pl.program_id(0)
    groups = pl.num_programs(0)
    length = x_ref.shape[0]
    taps = taps_ref.shape[0]
    xs[0:8, :] = edge_ref[...].astype(jnp.float32)
    xs[8 : 8 + length, :] = x_ref[...].astype(jnp.float32)
    rows = length // 4
    kernel = taps_ref[...].astype(jnp.float32)
    v = -soft_ref[...]
    soft = jnp.maximum(v, 0.0) + jnp.log1p(jnp.exp(-jnp.abs(v)))
    for at in range(0, length, rows):
        conv = jnp.zeros((rows, LANES), jnp.float32)
        for k in range(taps):
            first = 8 + at - (taps - 1) + k
            conv = conv + xs[first : first + rows, :] * kernel[k : k + 1, :]
        conv = conv.astype(jnp.bfloat16)
        rgate = sigmoid(jnp.dot(conv, rmap_ref[0], preferred_element_type=jnp.float32))
        igate = sigmoid(jnp.dot(conv, imap_ref[0], preferred_element_type=jnp.float32))
        log_decay = -GATE_SCALE * rgate * soft + jump_ref[at : at + rows, :]
        decay[at : at + rows, :] = jnp.exp(log_decay)
        drive[at : at + rows, :] = (
            jnp.sqrt(minus_expm1(2.0 * log_decay)) * igate * conv.astype(jnp.float32)
        )
    steps = length // SEGMENTS

    def step(i, carry):
        state, product = carry
        where = pl.ds(i, SEGMENTS, steps)
        a = decay[where, :]
        state = a * state + drive[where, :]
        product = a * product
        loc_ref[where, :] = state
        cum_ref[where, :] = product
        return state, product

    zero = jnp.zeros((SEGMENTS, LANES), jnp.float32)
    state, product = lax.fori_loop(0, steps, step, (zero, zero + 1.0), unroll=8)
    seg_ref[0, :, :] = product
    seg_ref[1, :, :] = state
    all_state = state[0:1]
    all_product = product[0:1]
    for s in range(1, SEGMENTS):
        all_state = product[s : s + 1] * all_state + state[s : s + 1]
        all_product = product[s : s + 1] * all_product
    count = ends_ref.shape[0]
    ends_ref[:, pl.ds(group, 1), :] = jnp.broadcast_to(all_product[None], (count, 1, LANES))
    ends_ref[:, pl.ds(groups + group, 1), :] = jnp.broadcast_to(all_state[None], (count, 1, LANES))


def local_scan(x, edge, taps, rmap, imap, soft, jump, copies):
    length, channels = x.shape
    groups = channels // LANES
    column = lambda rows: pl.BlockSpec((rows, LANES), lambda g: (0, g))
    square = pl.BlockSpec((1, LANES, LANES), lambda g: (g, 0, 0))
    return pl.pallas_call(
        scan_kernel,
        grid=(groups,),
        in_specs=[column(length), column(8), column(taps.shape[0]), square, square, column(1), column(length)],
        out_specs=[
            column(length),
            column(length),
            pl.BlockSpec((2, SEGMENTS, LANES), lambda g: (0, 0, g)),
            pl.BlockSpec((copies, 2 * groups, LANES), lambda g: (0, 0, 0)),
        ],
        out_shape=[
            jax.ShapeDtypeStruct((length, channels), jnp.float32),
            jax.ShapeDtypeStruct((length, channels), jnp.float32),
            jax.ShapeDtypeStruct((2, SEGMENTS, channels), jnp.float32),
            jax.ShapeDtypeStruct((copies, 2 * groups, LANES), jnp.float32),
        ],
        scratch_shapes=[
            pltpu.VMEM((length + 8, LANES), jnp.float32),
            pltpu.VMEM((length, LANES), jnp.float32),
            pltpu.VMEM((length, LANES), jnp.float32),
        ],
        name="local_scan",
    )(x, edge, taps, rmap, imap, soft, jump)


def branch_kernel(
    me_ref, arrived, seg, cum_hbm, loc_hbm, gate_hbm, w_ref, *rest, turns
):
    outs, (cum, loc, gates, carry, state, sems) = rest[:-6], rest[-6:]
    rows, channels = state.shape
    groups = channels // LANES
    per_block = SEGMENTS // BLOCKS
    seg_rows = rows // per_block
    starts = [lax.rem(me_ref[0] + steps, BLOCKS) for steps in turns]
    copies = []
    for b, block in enumerate(starts):
        at = pl.ds(pl.multiple_of(block * rows, rows), rows)
        for k, (source, target) in enumerate(((cum_hbm, cum), (loc_hbm, loc), (gate_hbm, gates))):
            copies.append(pltpu.make_async_copy(source.at[at, :], target.at[b], sems.at[3 * b + k]))
    for copy in copies:
        copy.start()

    def join(j, state):
        return arrived[j, 0:groups, :] * state + arrived[j, groups : 2 * groups, :]

    before = lax.fori_loop(0, me_ref[1], join, jnp.zeros((groups, LANES), jnp.float32))
    for g in range(groups):
        lanes = slice(g * LANES, (g + 1) * LANES)
        now = before[g : g + 1, :]
        for s in range(SEGMENTS):
            carry[s, 0:1, lanes] = now
            now = seg[0, s : s + 1, lanes] * now + seg[1, s : s + 1, lanes]
    for copy in copies:
        copy.wait()

    for b, block in enumerate(starts):
        for part in range(per_block):
            at = slice(part * seg_rows, (part + 1) * seg_rows)
            state[at, :] = loc[b, at, :] + cum[b, at, :] * carry[block * per_block + part, 0:1, :]
        out = (state[...] * gelu(gates[b].astype(jnp.float32))).astype(jnp.bfloat16)
        put(outs, b, turns[b], jnp.dot(out, w_ref[...], preferred_element_type=jnp.float32))


def put(outs, at, steps, share):
    share = share.astype(jnp.bfloat16)
    half = share.shape[1] // 2
    if steps:
        outs[2 * at][...] = share[:, :half]
        outs[2 * at + 1][...] = share[:, half:]
    else:
        outs[2 * at][...] = share


VMEM = pl.BlockSpec(memory_space=pltpu.VMEM)
HERE = pl.BlockSpec(memory_space=pltpu.HBM)
OPPOSITE, SIDES, OTHERS, OWN = (2,), (1, 3), (1, 3, 0), (0,)


def vm(value):
    return pltpu.with_memory_space_constraint(value, pltpu.VMEM)


def hbm(value):
    return pltpu.with_memory_space_constraint(value, pltpu.HBM)


def hbm_out(shape):
    return pltpu.HBM(shape, jnp.bfloat16)


def vm_out(shape):
    return pltpu.VMEM(shape, jnp.bfloat16)


def share_shapes(turns, rows, width):
    half = vm_out((rows, width // 2))
    return sum(([half] * 2 if steps else [vm_out((rows, width))] for steps in turns), [])


def branch_shares(me, arrived, seg, cum, loc, gate, weight, turns):
    length, channels = cum.shape
    width = weight.shape[1]
    rows = length // BLOCKS
    count = len(turns)
    out_shape = share_shapes(turns, rows, width)
    return pl.pallas_call(
        functools.partial(branch_kernel, turns=turns),
        in_specs=[pl.BlockSpec(memory_space=pltpu.SMEM), VMEM, VMEM, *[HERE] * 3, VMEM],
        out_specs=[VMEM] * len(out_shape),
        out_shape=out_shape,
        scratch_shapes=[
            pltpu.VMEM((count, rows, channels), jnp.float32),
            pltpu.VMEM((count, rows, channels), jnp.float32),
            pltpu.VMEM((count, rows, channels), jnp.bfloat16),
            pltpu.VMEM((SEGMENTS, 1, channels), jnp.float32),
            pltpu.VMEM((rows, channels), jnp.float32),
            pltpu.SemaphoreType.DMA((3 * count,)),
        ],
        cost_estimate=pl.CostEstimate(
            flops=2 * count * rows * channels * width,
            bytes_accessed=count * rows * (10 * channels + 2 * width) + 2 * channels * width,
            transcendentals=count * rows * channels,
        ),
        compiler_params=pltpu.CompilerParams(vmem_limit_bytes=16 * MIB),
        name="branch_first" if count == 1 else "branch_rest",
    )(me, arrived, seg, hbm(cum), hbm(loc), hbm(gate), weight)


def feed_kernel(*refs, turns):
    first = turns == OPPOSITE
    me_ref, outside = refs[:2]
    halves = {0: refs[2:4], 1: refs[4:6], 2: refs[6:8], 3: refs[8:10]}
    if first:
        weights, gk_ref, vk_ref, *outs, ring, down, lhs, up, act, sems = refs[10:]
    else:
        ring, down, gk_ref, vk_ref, *outs, lhs, up, act = refs[10:]
    rows = halves[0][0].shape[0]
    tall = rows + HALO
    taps = gk_ref.shape[0]
    shards, chunks, shard_rows, _ = down.shape
    width = shards * shard_rows
    half = width // 2
    columns = (slice(0, half), slice(half, width))

    def get(chunk):
        return pltpu.make_async_copy(weights.at[:, pl.ds(2 * chunk, 2)], ring.at[chunk], sems.at[chunk])

    def fill(b, steps):
        at = b * tall
        for part, behind in zip(columns, halves[(steps - 1) % BLOCKS]):
            lhs[at : at + HALO, part] = behind[rows - HALO : rows, :]

        @pl.when(lax.rem(me_ref[0] + steps, BLOCKS) == 0)
        def _():
            lhs[at : at + HALO, :] = outside[...]

        for part, own in zip(columns, halves[steps]):
            lhs[at + HALO : at + tall, part] = own[...]

    def activate(chunk):
        side = lax.rem(chunk, 2)
        lanes = pl.ds(pl.multiple_of(chunk * LANES, LANES), LANES)
        gate_taps = gk_ref[:, lanes].astype(jnp.float32)
        value_taps = vk_ref[:, lanes].astype(jnp.float32)
        for b in range(len(turns)):
            gate = jnp.zeros((rows, LANES), jnp.float32)
            value = jnp.zeros((rows, LANES), jnp.float32)
            for k in range(taps):
                at = b * tall + HALO - (taps - 1) + k
                gate = gate + up[side, at : at + rows, 0:LANES] * gate_taps[k : k + 1, :]
                value = value + up[side, at : at + rows, LANES : 2 * LANES] * value_taps[k : k + 1, :]
            act[b * rows : (b + 1) * rows, lanes] = (gelu(gate) * value).astype(jnp.bfloat16)

    def project(chunk):
        sides = [ring[chunk, :, side].reshape(width, LANES) for side in range(2)]
        up[lax.rem(chunk, 2)] = (
            jnp.dot(lhs[...], jnp.concatenate(sides, axis=1), preferred_element_type=jnp.float32)
            .astype(jnp.bfloat16)
            .astype(jnp.float32)
        )

    if first:
        get_down = pltpu.make_async_copy(weights.at[:, pl.ds(2 * chunks, chunks)], down, sems.at[chunks])
        for chunk in range(chunks):
            get(jnp.int32(chunk)).start()
        get_down.start()
    for b, steps in enumerate(turns):
        fill(b, steps)
    if first:
        get(jnp.int32(0)).wait()
    project(jnp.int32(0))

    def step(chunk, carry):
        if first:
            get(chunk + 1).wait()
        activate(chunk)
        project(chunk + 1)
        return carry

    lax.fori_loop(0, chunks - 1, step, 0)
    if first:
        get_down.wait()
    activate(jnp.int32(chunks - 1))
    turned = jnp.concatenate([down[:, c].reshape(width, LANES) for c in range(chunks)], axis=1)
    share = lax.dot_general(
        act[...], turned, (((1,), (1,)), ((), ())), preferred_element_type=jnp.float32
    )
    for b in range(len(turns)):
        put(outs, b, turns[b], share[b * rows : (b + 1) * rows, :])


def feed(me, outside, halves, weights, gate_kernel, value_kernel, turns):
    first = turns == OPPOSITE
    count = len(turns)
    rows, half = halves[0].shape
    width, units = 2 * half, gate_kernel.shape[1]
    chunks = units // LANES
    tall = count * (rows + HALO)
    out_shape = share_shapes(turns, rows, width)
    scratch = [
        pltpu.VMEM((tall, width), jnp.bfloat16),
        pltpu.VMEM((2, tall, 2 * LANES), jnp.float32),
        pltpu.VMEM((count * rows, units), jnp.bfloat16),
    ]
    if first:
        shards, _, shard_rows, _ = weights[0].shape
        out_shape += [
            vm_out((chunks, shards, 2, shard_rows, LANES)),
            vm_out((shards, chunks, shard_rows, LANES)),
        ]
        scratch += [pltpu.SemaphoreType.DMA((chunks + 1,))]
    else:
        weights = map(vm, weights)
    return pl.pallas_call(
        functools.partial(feed_kernel, turns=turns),
        in_specs=[
            pl.BlockSpec(memory_space=pltpu.SMEM),
            *[VMEM] * (1 + len(halves)),
            *([HERE] if first else [VMEM] * 2),
            VMEM,
            VMEM,
        ],
        out_specs=[VMEM] * len(out_shape),
        out_shape=out_shape,
        scratch_shapes=scratch,
        cost_estimate=pl.CostEstimate(
            flops=6 * count * rows * width * units,
            bytes_accessed=6 * width * units + 4 * count * rows * width,
            transcendentals=count * rows * units,
        ),
        compiler_params=pltpu.CompilerParams(vmem_limit_bytes=12 * MIB),
    )(me, outside, *map(vm, halves[:4]), *halves[4:6], *map(vm, halves[6:]), *weights, gate_kernel, value_kernel)


def pack_kernel(gate_ref, value_ref, turned_ref, out_ref, sems):
    chunks = gate_ref.shape[1] // LANES
    copies = []
    for c in range(chunks):
        lanes = pl.ds(c * LANES, LANES)
        for source, at in ((gate_ref, 2 * c), (value_ref, 2 * c + 1), (turned_ref, 2 * chunks + c)):
            copies.append(pltpu.make_async_copy(source.at[:, lanes], out_ref.at[at], sems.at[at]))
    for copy in copies:
        copy.start()
    for copy in copies:
        copy.wait()


def packed(gate, value, turned):
    rows, units = gate.shape
    pieces = 3 * units // LANES
    return pl.pallas_call(
        pack_kernel,
        in_specs=[HERE] * 3,
        out_specs=HERE,
        out_shape=hbm_out((pieces, rows, LANES)),
        scratch_shapes=[pltpu.SemaphoreType.DMA((pieces,))],
        name="pack",
    )(hbm(gate), hbm(value), hbm(turned))


def scaled(v, gain):
    return v * lax.rsqrt(jnp.mean(v * v, axis=-1, keepdims=True) + EPS) * gain


def shares_sum(refs, at):
    own, left_low, left_high, right_low, right_high = refs
    half = left_low.shape[1]
    parts = []
    for part, left, right in (
        (slice(0, half), left_low, right_low),
        (slice(half, 2 * half), left_high, right_high),
    ):
        total = own[at, part].astype(jnp.float32) + left[at, :].astype(jnp.float32)
        total = total + right[at, :].astype(jnp.float32)
        parts.append(total.astype(jnp.bfloat16).astype(jnp.float32))
    return jnp.concatenate(parts, axis=1)


def by_rows(rows, body):
    def step(i, carry):
        body(pl.ds(pl.multiple_of(i * HALO, HALO), HALO))
        return carry

    lax.fori_loop(0, rows // HALO, step, 0)


def mid_kernel(me_ref, *refs):
    shares, (res_ref, mix_ref, inner_ref, hidden_ref, low_ref, high_ref) = refs[:5], refs[5:]
    rows, half = low_ref.shape
    first = me_ref[0] * rows
    mix, inner = mix_ref[...], inner_ref[...]

    def body(at):
        there = pl.ds(pl.multiple_of(first + at.start, HALO), HALO)
        hidden = (
            res_ref[there, :].astype(jnp.float32) + scaled(shares_sum(shares, at), mix)
        ).astype(jnp.bfloat16)
        hidden_ref[at, :] = hidden
        normed = scaled(hidden.astype(jnp.float32), inner).astype(jnp.bfloat16)
        low_ref[at, :] = normed[:, :half]
        high_ref[at, :] = normed[:, half:]

    by_rows(rows, body)


def mid(me, shares, residual, mix_gain, inner_gain):
    rows, width = shares[0].shape
    return pl.pallas_call(
        mid_kernel,
        in_specs=[pl.BlockSpec(memory_space=pltpu.SMEM), *[VMEM] * 8],
        out_specs=[VMEM] * 3,
        out_shape=[
            hbm_out((rows, width)),
            *[vm_out((rows, width // 2))] * 2,
        ],
        compiler_params=pltpu.CompilerParams(vmem_limit_bytes=12 * MIB),
        name="mid",
    )(me, *map(vm, shares), residual, mix_gain, inner_gain)


def last_kernel(*refs):
    shares, (hidden_ref, gain_ref, out_ref) = refs[:5], refs[5:]
    gain = gain_ref[...]

    def body(at):
        out_ref[at, :] = (
            hidden_ref[at, :].astype(jnp.float32) + scaled(shares_sum(shares, at), gain)
        ).astype(jnp.bfloat16)

    by_rows(hidden_ref.shape[0], body)


def last(shares, hidden, gain):
    return pl.pallas_call(
        last_kernel,
        in_specs=[VMEM] * 7,
        out_specs=VMEM,
        out_shape=jax.ShapeDtypeStruct(hidden.shape, jnp.bfloat16),
        compiler_params=pltpu.CompilerParams(vmem_limit_bytes=12 * MIB),
        name="last",
    )(*map(vm, shares), hidden, gain)


def join_kernel(right_low, low_ref, left_high, high_ref, right_ref, left_ref):
    def body(at):
        for own, other, out in ((right_low, low_ref, right_ref), (left_high, high_ref, left_ref)):
            total = own[at, :].astype(jnp.float32) + other[at, :].astype(jnp.float32)
            out[at, :] = total.astype(jnp.bfloat16)

    by_rows(low_ref.shape[0], body)


def join(right_low, low, left_high, high):
    return pl.pallas_call(
        join_kernel,
        in_specs=[VMEM] * 4,
        out_specs=[VMEM] * 2,
        out_shape=[vm_out(low.shape)] * 2,
        compiler_params=pltpu.CompilerParams(vmem_limit_bytes=12 * MIB),
        name="join",
    )(*map(vm, (right_low, low, left_high, high)))


def turn(value, axis, steps):
    count = lax.axis_size(axis)
    return lax.ppermute(value, axis, [(i, (i + steps) % count) for i in range(count)])


def ring_sum(first, rest):
    low, high = turn(first[0], "tp", 1), turn(first[1], "tp", -1)
    right_low, right_high, left_low, left_high, own = rest
    from_left_high, from_right_low = turn(right_high, "tp", 1), turn(left_low, "tp", -1)
    right_low, left_high = join(right_low, low, left_high, high)
    from_left_low, from_right_high = turn(right_low, "tp", 1), turn(left_high, "tp", -1)
    return own, from_left_low, from_left_high, from_right_low, from_right_high


def from_behind(value, axis):
    count = lax.axis_size(axis)
    return lax.ppermute(value, axis, [(i, i + 1) for i in range(count - 1)])


def tail_sent(value, pairs):
    return lax.ppermute(value, ("sp", "tp"), pairs)


def exchanged(tiles, axis):
    return lax.all_to_all(tiles, axis, split_axis=0, concat_axis=0, tiled=True)


def local(
    residual,
    mix_input,
    gate_input,
    mix_kernel,
    recur_gate_map,
    input_gate_map,
    decay_param,
    jump_log,
    out_weight,
    mix_gain,
    inner_gain,
    final_gain,
    gate_weight,
    value_weight,
    gate_kernel,
    value_kernel,
    down_weight,
):
    n_tp, n_sp = lax.axis_size("tp"), lax.axis_size("sp")
    assert n_tp == BLOCKS
    tp_me = lax.axis_index("tp").astype(jnp.int32)
    me = jnp.stack([tp_me, lax.axis_index("sp").astype(jnp.int32)])

    edge = from_behind(mix_input[mix_input.shape[0] - 8 :], "sp")
    shard = packed(gate_weight, value_weight, down_weight.T)
    weights = lax.all_gather(shard, "sp", axis=0, tiled=True).reshape(n_sp, *shard.shape)

    cum, loc, seg, ends = local_scan(
        mix_input, edge, mix_kernel, recur_gate_map, input_gate_map, decay_param[None], jump_log, n_sp
    )
    arrived = exchanged(ends, "sp")
    shares = functools.partial(
        branch_shares, arrived=arrived, seg=seg, cum=cum, loc=loc, gate=gate_input, weight=out_weight
    )
    first = shares(me, turns=OPPOSITE)
    rest = shares(me, turns=OTHERS)
    hidden_state, own_low, own_high = mid(
        me, ring_sum(first, rest), residual, mix_gain[None], inner_gain[None]
    )
    left_low, right_high = turn(own_low, "tp", 1), turn(own_high, "tp", -1)
    left_high, right_low = turn(own_high, "tp", 1), turn(own_low, "tp", -1)
    opposite_low, opposite_high = turn(left_low, "tp", 1), turn(right_high, "tp", -1)

    tail = lambda low, high: jnp.concatenate([low[-HALO:], high[-HALO:]], axis=1)
    own_tail = tail(own_low, own_high)
    final_tail = jnp.where(
        tp_me == n_tp - 1,
        own_tail,
        jnp.where(tp_me == 0, tail(left_low, left_high), tail(right_low, right_high)),
    )
    places = range(n_sp - 1)
    outside = jnp.where(
        tp_me == 1,
        tail_sent(own_tail, [(s * n_tp + n_tp - 1, (s + 1) * n_tp + 1) for s in places]),
        tail_sent(
            final_tail,
            [(s * n_tp + t, (s + 1) * n_tp + t) for s in places for t in (0, 2, 3)],
        ),
    )
    halves = (own_low, own_high, right_low, right_high, opposite_low, opposite_high, left_low, left_high)
    *first, ring, down = feed(
        me, outside, halves, (hbm(weights),), gate_kernel, value_kernel, turns=OPPOSITE
    )
    given = (me, outside, halves, (ring, down), gate_kernel, value_kernel)
    rest = feed(*given, turns=SIDES) + feed(*given, turns=OWN)
    return last(ring_sum(first, rest), hidden_state, final_gain[None])


def solution(mesh):
    return jax.shard_map(
        local,
        mesh=mesh,
        in_specs=(
            P(("grp", "sp"), None),
            P(("grp", "sp"), "tp"),
            P(("grp", "sp"), "tp"),
            P(None, "tp"),
            P("tp", None, None),
            P("tp", None, None),
            P("tp"),
            P(("grp", "sp"), "tp"),
            P("tp", None),
            P(),
            P(),
            P(),
            P("sp", "tp"),
            P("sp", "tp"),
            P(None, "tp"),
            P(None, "tp"),
            P("tp", "sp"),
        ),
        out_specs=P(("grp", "sp", "tp"), None),
        check_vma=False,
    )
```
